256 devices in a mesh: sp: 64 (over z, y, core), tp: 4 (over x).
Axes of the slice: x: 4, y: 4, z: 8, core: 2. Of those that a mesh axis runs over, the one named last changes fastest.
Arguments:
- tokens: bfloat16 [16384, 2048], P('sp', 'tp'), may hold values from -6 to 6
- in_gain: float32 [2048], replicated, may hold values from 0.1 to 1.9
- query_down: bfloat16 [2048, 512], replicated, may hold values from -0.125 to 0.125
- latent_down: bfloat16 [2048, 256], replicated, may hold values from -0.125 to 0.125
- rope_down: bfloat16 [2048, 32], replicated, may hold values from -0.125 to 0.125
- query_gain: float32 [512], replicated, may hold values from 0.5 to 12
- latent_gain: float32 [256], replicated, may hold values from 0.5 to 12
- query_nope: bfloat16 [512, 1024], P(None, 'tp'), may hold values from -0.25 to 0.25
- query_rope: bfloat16 [512, 512], P(None, 'tp'), may hold values from -0.25 to 0.25
- key_up: bfloat16 [256, 1024], P(None, 'tp'), may hold values from -0.375 to 0.375
- value_up: bfloat16 [256, 1024], P(None, 'tp'), may hold values from -0.375 to 0.375
- conv_value: bfloat16 [2048, 2048], P(None, 'tp'), may hold values from -0.125 to 0.125
- conv_gate: bfloat16 [2048, 2048], P(None, 'tp'), may hold values from -0.125 to 0.125
- conv_taps: float32 [31, 2048], P(None, 'tp'), may hold values from -1 to 1
- conv_bias: float32 [2048], P('tp'), may hold values from 0.05 to 2.25
- channel_gain: float32 [2048], P('tp'), may hold values from 0.1 to 1.9
- out_attend: bfloat16 [1024, 2048], P('tp'), may hold values from -0.109375 to 0.109375
- out_conv: bfloat16 [2048, 2048], P('tp'), may hold values from -0.109375 to 0.109375
Outputs:
- mixed: bfloat16 [16384, 2048], P('sp', 'tp')
The draws below stay inside these ranges and needn't reach their ends.
All inputs are finite; a program needn't handle non-finite values.
Results may differ from the reference program's by a relative error of at most 0.013.
The reference program's roundings to bfloat16 on the way count: a program that leaves them out, or rounds other values in their place, can miss the bound.
Values may be sent and summed in bfloat16 or wider, within the bound.
A program may use at most 128 MiB of HBM per device.

```python
import math
import jax
import jax.numpy as jnp
from jax import lax

D = 2048
HEADS = 16
NOPE = 64
ROPE = 32
VDIM = 64
QRANK = 512
KVRANK = 256
CONV_CH = 2048
KWIDTH = 31
SEQ = 16384
GROUPS = 4


def draw_query_gain(key, part):
    return jax.random.uniform(key, (QRANK,), jnp.float32, 0.5, 1.5)


def draw_latent_gain(key, part):
    return jax.random.uniform(key, (KVRANK,), jnp.float32, 0.5, 1.5)


def draw_conv_bias(key, part):
    factor = jax.random.uniform(key, (CONV_CH,), jnp.float32, 0.5, 1.5)
    ramp = jnp.arange(CONV_CH).astype(jnp.float32) / (CONV_CH - 1)
    level = 0.1 + 0.9 * ramp
    return level * factor


def level_of(rng, extent, pieces, low, top_value):
    level, own = 1.0, jax.random.fold_in(rng, 6)
    for dim, blocks in pieces:
        draws = jnp.exp(jax.random.uniform(jax.random.fold_in(own, dim), (blocks,), jnp.float32, low / len(pieces), top_value / len(pieces)))
        level = level * jnp.repeat(draws, extent[dim] // blocks).reshape([-1 if axis == dim else 1 for axis in range(len(extent))])
    return level


def normal_values(rng, shape, deviation, most, shards=(), kind=jnp.bfloat16):
    result = deviation * jax.random.normal(rng, shape, jnp.float32)
    if shards:
        result = result * level_of(rng, shape, shards, -0.22, 0.18)
    return jnp.clip(result, -most, most).astype(kind)


def setup_inputs(seed: int = 0) -> dict:
    key_of = jax.random.split(jax.random.key(seed), 19)
    tokens = normal_values(key_of[0], (SEQ, D), 1.0, 6.0, ((0, 64), (1, 4)))
    in_gain = jnp.clip(1.0 + 0.18 * jax.random.normal(key_of[1], (D,), jnp.float32), 0.1, 1.9)
    query_down = normal_values(key_of[2], (D, QRANK), D ** -0.5, 0.125)
    latent_down = normal_values(key_of[3], (D, KVRANK), D ** -0.5, 0.125)
    rope_down = normal_values(key_of[4], (D, ROPE), D ** -0.5, 0.125)
    query_gain = draw_query_gain(jax.random.fold_in(key_of[18], 71), 0)
    latent_gain = draw_latent_gain(jax.random.fold_in(key_of[18], 71), 0)
    query_nope = normal_values(key_of[7], (QRANK, HEADS * NOPE), QRANK ** -0.5, 0.25, ((1, 4),))
    query_rope = normal_values(key_of[8], (QRANK, HEADS * ROPE), QRANK ** -0.5, 0.25, ((1, 4),))
    key_up = normal_values(key_of[9], (KVRANK, HEADS * NOPE), KVRANK ** -0.5, 0.375, ((1, 4),))
    value_up = normal_values(key_of[10], (KVRANK, HEADS * VDIM), KVRANK ** -0.5, 0.375, ((1, 4),))
    conv_value = normal_values(key_of[11], (D, CONV_CH), D ** -0.5, 0.125, ((1, 4),))
    conv_gate = normal_values(key_of[12], (D, CONV_CH), D ** -0.5, 0.125, ((1, 4),))
    conv_taps = normal_values(key_of[13], (KWIDTH, CONV_CH), KWIDTH ** -0.5, 1.0, ((1, 4),), jnp.float32)
    conv_bias = draw_conv_bias(jax.random.fold_in(key_of[18], 71), 0)
    channel_gain = jnp.clip(1.0 + 0.18 * jax.random.normal(key_of[15], (CONV_CH,), jnp.float32), 0.1, 1.9)
    out_attend = normal_values(key_of[16], (HEADS * VDIM, D), (HEADS * VDIM + CONV_CH) ** -0.5, 0.109375, ((0, 4),))
    out_conv = normal_values(key_of[17], (CONV_CH, D), (HEADS * VDIM + CONV_CH) ** -0.5, 0.109375, ((0, 4),))
    return dict(tokens=tokens, in_gain=in_gain, query_down=query_down, latent_down=latent_down, rope_down=rope_down, query_gain=query_gain, latent_gain=latent_gain, query_nope=query_nope, query_rope=query_rope, key_up=key_up, value_up=value_up, conv_value=conv_value, conv_gate=conv_gate, conv_taps=conv_taps, conv_bias=conv_bias, channel_gain=channel_gain, out_attend=out_attend, out_conv=out_conv)


eps_norm = 1e-06
eps_layer = 1e-05
theta = 10000.0

def rms_scale(values, gain):
    return values * lax.rsqrt(lax.optimization_barrier(jnp.mean(values * values, axis=-1, keepdims=True)) + eps_norm) * gain

def rotate(values, positions):
    half = values.shape[-1] // 2
    freqs = theta ** (-jnp.arange(half).astype(jnp.float32) / half)
    angles = positions[..., None] * freqs
    cosine = jnp.cos(angles)
    sine = jnp.sin(angles)
    first = values[..., :half]
    second = values[..., half:]
    return jnp.concatenate([first * cosine - second * sine, second * cosine + first * sine], axis=-1)

def reference(tokens, in_gain, query_down, latent_down, rope_down, query_gain, latent_gain, query_nope, query_rope, key_up, value_up, conv_value, conv_gate, conv_taps, conv_bias, channel_gain, out_attend, out_conv):
    tokens_f = tokens.astype(jnp.float32)
    row_scale = lax.rsqrt(lax.optimization_barrier(jnp.mean(tokens_f * tokens_f, axis=-1, keepdims=True)) + eps_norm)
    scaled = (tokens_f * in_gain).astype(jnp.bfloat16)
    positions = jnp.arange(SEQ).astype(jnp.float32)

    def project(weight):
        return row_scale * jnp.dot(scaled, weight, preferred_element_type=jnp.float32)
    q_latent = rms_scale(project(query_down), query_gain).astype(jnp.bfloat16)
    kv_latent = rms_scale(project(latent_down), latent_gain).astype(jnp.bfloat16)
    rope_key = rotate(project(rope_down), positions).astype(jnp.bfloat16)
    q_nope = jnp.dot(q_latent, query_nope, preferred_element_type=jnp.float32).astype(jnp.bfloat16)
    q_turn = jnp.dot(q_latent, query_rope, preferred_element_type=jnp.float32).reshape(SEQ, HEADS, ROPE)
    q_rope = rotate(q_turn, positions[:, None]).astype(jnp.bfloat16)
    k_nope = jnp.dot(kv_latent, key_up, preferred_element_type=jnp.float32).astype(jnp.bfloat16)
    values = jnp.dot(kv_latent, value_up, preferred_element_type=jnp.float32).astype(jnp.bfloat16)
    key_heads = k_nope.astype(jnp.float32).reshape(SEQ, HEADS, NOPE)
    value_heads = values.astype(jnp.float32).reshape(SEQ, HEADS, VDIM)
    rope_f = rope_key.astype(jnp.float32)
    score_scale = (NOPE + ROPE) ** (-0.5)
    block = math.gcd(SEQ, 256)
    q_blocks = q_nope.reshape(SEQ // block, block, HEADS, NOPE)
    r_blocks = q_rope.reshape(SEQ // block, block, HEADS, ROPE)

    def attend(pair):
        q_part = pair[0].astype(jnp.float32)
        r_part = pair[1].astype(jnp.float32)
        scores = (jnp.einsum('qhd,khd->hqk', q_part, key_heads) + jnp.einsum('qhd,kd->hqk', r_part, rope_f)) * score_scale
        highest = lax.optimization_barrier(jnp.max(scores, axis=-1, keepdims=True))
        weight = jnp.exp(scores - highest)
        total = lax.optimization_barrier(jnp.sum(weight, axis=-1))
        rounded = lax.optimization_barrier(weight.astype(jnp.bfloat16)).astype(jnp.float32)
        summed = jnp.einsum('hqk,khd->qhd', rounded, value_heads)
        return (summed / jnp.transpose(total)[:, :, None]).astype(jnp.bfloat16)
    attended = lax.map(attend, (q_blocks, r_blocks)).reshape(SEQ, HEADS * VDIM)
    glu = (project(conv_value) * jax.nn.sigmoid(project(conv_gate))).astype(jnp.bfloat16)
    half = KWIDTH // 2
    padded = jnp.pad(glu.astype(jnp.float32), ((half, half), (0, 0)))
    conv = jnp.zeros((SEQ, CONV_CH), jnp.float32) + conv_bias
    for tap in range(KWIDTH):
        conv = conv + conv_taps[tap] * padded[tap:tap + SEQ]
    mean = lax.optimization_barrier(jnp.mean(conv, axis=-1, keepdims=True))
    centred = conv - mean
    spread = lax.optimization_barrier(jnp.mean(centred * centred, axis=-1, keepdims=True))
    activated = jax.nn.silu(centred * lax.rsqrt(spread + eps_layer) * channel_gain).astype(jnp.bfloat16)
    head_cols = HEADS * VDIM // GROUPS
    chan_cols = CONV_CH // GROUPS
    mixed = jnp.zeros((SEQ, D), jnp.float32)
    for group in range(GROUPS):
        part_attend = jnp.dot(attended[:, group * head_cols:(group + 1) * head_cols], out_attend[group * head_cols:(group + 1) * head_cols], preferred_element_type=jnp.float32)
        part_conv = jnp.dot(activated[:, group * chan_cols:(group + 1) * chan_cols], out_conv[group * chan_cols:(group + 1) * chan_cols], preferred_element_type=jnp.float32)
        mixed = mixed + (part_attend + part_conv).astype(jnp.bfloat16).astype(jnp.float32)
    return mixed.astype(jnp.bfloat16)
```

```python
import functools
import math

import jax
import jax.numpy as jnp
from jax import lax
from jax.experimental import pallas as pl
from jax.experimental.pallas import tpu as pltpu
from jax.sharding import PartitionSpec as P

eps_norm = 1e-06
eps_layer = 1e-05
theta = 10000.0
bf16 = jnp.bfloat16
f32 = jnp.float32

CHUNKS = 4


def laid_out(blocks, dim):
    dims = list(blocks.shape[1:])
    dims[dim] *= blocks.shape[0]
    return jnp.moveaxis(blocks, 0, dim).reshape(dims)


def sent_to_all(shard, axis):
    copies = jnp.broadcast_to(shard, (lax.axis_size(axis), *shard.shape))
    return lax.all_to_all(copies, axis, split_axis=0, concat_axis=0, tiled=True)


def gather_directly(shard, axis, dim):
    return laid_out(sent_to_all(shard, axis), dim)


def padded_2(cells, sides, width):
    for axis, dim in sides:
        count = lax.axis_size(axis)
        ends = count - 1
        head = lax.slice_in_dim(cells, 0, width, axis=dim)
        tail = lax.slice_in_dim(cells, cells.shape[dim] - width, cells.shape[dim], axis=dim)
        cells = jnp.concatenate(
            [
                lax.ppermute(tail, axis, [(i, (i + 1) % count) for i in range(ends)]),
                cells,
                lax.ppermute(head, axis, [((i + 1) % count, i) for i in range(ends)]),
            ],
            axis=dim,
        )
    return cells


def cut_along(shard, dim, peers):
    dims = shard.shape
    blocks = shard.reshape(*dims[:dim], peers, dims[dim] // peers, *dims[dim + 1 :])
    return jnp.moveaxis(blocks, dim, 0)


def sum_at_owner(shard, axis, dim):
    blocks = cut_along(shard, dim, lax.axis_size(axis))
    arrived = lax.all_to_all(blocks, axis, split_axis=0, concat_axis=0, tiled=True)
    return arrived.astype(f32).sum(axis=0)


def rms_scale(values, gain):
    return values * lax.rsqrt(jnp.mean(values * values, axis=-1, keepdims=True) + eps_norm) * gain


def rotate(values, positions):
    half = values.shape[-1] // 2
    freqs = theta ** (-jnp.arange(half).astype(f32) / half)
    angles = positions[..., None] * freqs
    cosine = jnp.cos(angles)
    sine = jnp.sin(angles)
    first = values[..., :half]
    second = values[..., half:]
    return jnp.concatenate(
        [first * cosine - second * sine, second * cosine + first * sine], axis=-1
    )


def attend_kernel(heads, nope, rope, first, x_ref, qt_ref, ku_ref, vut_ref, e_ref, *refs):
    if first:
        acc_ref, stat_ref = refs
    else:
        acc_in, stat_in, acc_ref, stat_ref = refs
    scale = math.log2(math.e) * (nope + rope) ** (-0.5)
    rank = ku_ref.shape[0]

    @pl.when(pl.program_id(0) == 0)
    def _():
        if first:
            acc_ref[...] = jnp.zeros_like(acc_ref)
            stat_ref[...] = jnp.zeros_like(stat_ref)
            stat_ref[0] = jnp.full(stat_ref.shape[1:], -jnp.inf, f32)
        else:
            acc_ref[...] = acc_in[...]
            stat_ref[...] = stat_in[...]

    latent = x_ref[:, :rank]
    k = jnp.dot(latent, ku_ref[...], preferred_element_type=f32).astype(bf16)
    spread = jnp.dot(x_ref[:, rank:], e_ref[...], preferred_element_type=f32).astype(bf16)
    vt = lax.dot_general(
        vut_ref[...], latent, (((1,), (1,)), ((), ())), preferred_element_type=f32
    ).astype(bf16)
    lane = lax.broadcasted_iota(jnp.int32, spread.shape, 1)
    for h in range(heads):
        pair = k[:, 128 * (h // 2) : 128 * (h // 2) + 128]
        mask = (lane < 64) if h % 2 == 0 else (lane >= 64)
        kh = jnp.where(mask, pair, spread)
        s = jnp.dot(kh, qt_ref[h], preferred_element_type=f32)
        old = stat_ref[0, h : h + 1, :]
        new = jnp.maximum(old, jnp.max(s, axis=0, keepdims=True))
        alpha = jnp.exp2((old - new) * scale)
        p = jnp.exp2((s - new) * scale)
        stat_ref[0, h : h + 1, :] = new
        stat_ref[1, h : h + 1, :] = stat_ref[1, h : h + 1, :] * alpha + jnp.sum(
            p, axis=0, keepdims=True
        )
        rows = vt.shape[0] // heads
        acc_ref[h] = acc_ref[h] * alpha + jnp.dot(
            vt[h * rows : (h + 1) * rows], p.astype(bf16), preferred_element_type=f32
        )


def attend(x, qt, key_up, value_up_t, expand, state, nope, rope, block):
    heads, _, queries = qt.shape
    vdim = value_up_t.shape[0] // heads
    count = x.shape[0]
    first = state is None
    whole = lambda a: pl.BlockSpec(a.shape, lambda i: (0,) * a.ndim)
    shapes = (
        jax.ShapeDtypeStruct((heads, vdim, queries), f32),
        jax.ShapeDtypeStruct((2, heads, queries), f32),
    )
    consts = (qt, key_up, value_up_t, expand)
    extra = () if first else state
    return pl.pallas_call(
        functools.partial(attend_kernel, heads, nope, rope, first),
        out_shape=shapes,
        grid=(count // block,),
        in_specs=[pl.BlockSpec((block, x.shape[1]), lambda i: (i, 0))]
        + [whole(a) for a in consts + extra],
        out_specs=tuple(whole(a) for a in shapes),
        cost_estimate=pl.CostEstimate(
            flops=2 * count * queries * heads * 320,
            bytes_accessed=count * 600,
            transcendentals=count * queries * heads,
        ),
        name="attend",
    )(x, *consts, *extra)


def per_device(
    tokens,
    in_gain,
    query_down,
    latent_down,
    rope_down,
    query_gain,
    latent_gain,
    query_nope,
    query_rope,
    key_up,
    value_up,
    conv_value,
    conv_gate,
    conv_taps,
    conv_bias,
    channel_gain,
    out_attend,
    out_conv,
):
    sp = lax.axis_size("sp")
    row_count = tokens.shape[0]
    width = in_gain.shape[0]
    local_ch = conv_value.shape[1]
    positions = (lax.axis_index("sp") * row_count + jnp.arange(row_count)).astype(f32)
    piece_f = gather_directly(tokens, "tp", 1).astype(f32)
    scaled = (piece_f * in_gain).astype(bf16)

    def add_rows(weight):
        return jnp.dot(scaled, weight, preferred_element_type=f32)

    square_sum = jnp.sum(piece_f * piece_f, axis=1)
    q_pre = add_rows(query_down)
    kv_pre = add_rows(latent_down)
    rope_pre = add_rows(rope_down)
    value_pre = add_rows(conv_value)
    gate_pre = add_rows(conv_gate)
    row_scale = lax.rsqrt(square_sum / width + eps_norm)[:, None]
    q_latent = rms_scale(row_scale * q_pre, query_gain).astype(bf16)
    kv_latent = rms_scale(row_scale * kv_pre, latent_gain).astype(bf16)
    rope_key = rotate(row_scale * rope_pre, positions).astype(bf16)
    rope_size = rope_down.shape[1]
    heads = query_rope.shape[1] // rope_size
    nope = query_nope.shape[1] // heads

    x = jnp.concatenate([kv_latent, rope_key], axis=1)
    groups = [list(range(c, sp, 2)) for c in range(2)]
    part = row_count // CHUNKS
    gathered = [
        lax.all_gather(
            x[i * part : (i + 1) * part],
            "sp",
            axis=0,
            tiled=True,
            axis_index_groups=groups,
        )
        for i in range(CHUNKS)
    ]

    q_heads = (
        jnp.dot(q_latent, query_nope, preferred_element_type=f32)
        .astype(bf16)
        .reshape(row_count, heads, nope)
    )
    q_turn = jnp.dot(q_latent, query_rope, preferred_element_type=f32).reshape(
        row_count, heads, rope_size
    )
    r_heads = rotate(q_turn, positions[:, None]).astype(bf16)
    empty = jnp.zeros((row_count, 64 - rope_size), bf16)
    cols = []
    for h in range(heads):
        if h % 2 == 0:
            cols += [q_heads[:, h], r_heads[:, h], empty]
        else:
            cols += [r_heads[:, h], empty, q_heads[:, h]]
    q_own = jnp.transpose(jnp.concatenate(cols, axis=1))
    swap = [(i, i ^ 1) for i in range(sp)]
    q_other = lax.ppermute(q_own, "sp", swap)
    qt = jnp.concatenate([q_own, q_other], axis=1).reshape(heads, 128, 2 * row_count)
    expand = jnp.tile(jnp.eye(rope_size, dtype=bf16), (1, 128 // rope_size))
    state = None
    for i in range(CHUNKS):
        state = attend(
            gathered[i], qt, key_up, jnp.transpose(value_up), expand, state, nope, rope_size, 512
        )
    acc, stat = state
    acc_other = lax.ppermute(acc[:, :, row_count:], "sp", swap)
    stat_other = lax.ppermute(stat[:, :, row_count:], "sp", swap)
    acc, stat = acc[:, :, :row_count], stat[:, :, :row_count]
    scale = (nope + rope_size) ** (-0.5)
    high = jnp.maximum(stat[0], stat_other[0])
    a, b = jnp.exp((stat[0] - high) * scale), jnp.exp((stat_other[0] - high) * scale)
    total = stat[1] * a + stat_other[1] * b
    merged = (acc * a[:, None] + acc_other * b[:, None]) / total[:, None]
    attended = merged.astype(bf16).reshape(-1, row_count)

    glu = (row_scale * value_pre * jax.nn.sigmoid(row_scale * gate_pre)).astype(bf16)
    taps = conv_taps.shape[0]
    padded = padded_2(glu, (("sp", 0),), taps // 2).astype(f32)
    conv = jnp.zeros((row_count, local_ch), f32) + conv_bias
    for tap in range(taps):
        conv = conv + conv_taps[tap] * padded[tap : tap + row_count]
    peers = lax.axis_size("tp")
    channels = local_ch * peers
    own_mean = jnp.mean(conv, axis=-1)
    off = conv - own_mean[:, None]
    own_spread = jnp.sum(off * off, axis=-1)
    sums = sent_to_all(jnp.stack([own_mean, own_spread]), "tp")
    means = sums[:, 0]
    mean = jnp.mean(means, axis=0)
    apart = means - mean
    spread = (jnp.sum(sums[:, 1], axis=0) + local_ch * jnp.sum(apart * apart, axis=0)) / channels
    centred = conv - mean[:, None]
    activated = jax.nn.silu(
        centred * lax.rsqrt(spread[:, None] + eps_layer) * channel_gain
    ).astype(bf16)
    summed = sum_at_owner(
        (
            lax.dot_general(
                out_attend, attended, (((0,), (0,)), ((), ())), preferred_element_type=f32
            )
            + lax.dot_general(
                out_conv, activated, (((0,), (1,)), ((), ())), preferred_element_type=f32
            )
        ).astype(bf16),
        "tp",
        0,
    )
    return jnp.transpose(summed).astype(bf16)


def solution(mesh):
    in_specs = (
        P("sp", "tp"),
        P(),
        P(),
        P(),
        P(),
        P(),
        P(),
        P(None, "tp"),
        P(None, "tp"),
        P(None, "tp"),
        P(None, "tp"),
        P(None, "tp"),
        P(None, "tp"),
        P(None, "tp"),
        P("tp"),
        P("tp"),
        P("tp", None),
        P("tp", None),
    )
    return jax.shard_map(
        per_device, mesh=mesh, in_specs=in_specs, out_specs=P("sp", "tp"), check_vma=False
    )
```

```python
import functools
import math

import jax
import jax.numpy as jnp
from jax import lax
from jax.experimental import pallas as pl
from jax.experimental.pallas import tpu as pltpu
from jax.sharding import PartitionSpec as P

eps_norm = 1e-06
eps_layer = 1e-05
theta = 10000.0
bf16 = jnp.bfloat16
f32 = jnp.float32

def laid_out(blocks, dim):
    dims = list(blocks.shape[1:])
    dims[dim] *= blocks.shape[0]
    return jnp.moveaxis(blocks, 0, dim).reshape(dims)


def sent_to_all(shard, axis):
    copies = jnp.broadcast_to(shard, (lax.axis_size(axis), *shard.shape))
    return lax.all_to_all(copies, axis, split_axis=0, concat_axis=0, tiled=True)


def gather_directly(shard, axis, dim):
    return laid_out(sent_to_all(shard, axis), dim)


def padded_2(cells, sides, width):
    for axis, dim in sides:
        count = lax.axis_size(axis)
        ends = count - 1
        head = lax.slice_in_dim(cells, 0, width, axis=dim)
        tail = lax.slice_in_dim(cells, cells.shape[dim] - width, cells.shape[dim], axis=dim)
        cells = jnp.concatenate(
            [
                lax.ppermute(tail, axis, [(i, (i + 1) % count) for i in range(ends)]),
                cells,
                lax.ppermute(head, axis, [((i + 1) % count, i) for i in range(ends)]),
            ],
            axis=dim,
        )
    return cells


def cut_along(shard, dim, peers):
    dims = shard.shape
    blocks = shard.reshape(*dims[:dim], peers, dims[dim] // peers, *dims[dim + 1 :])
    return jnp.moveaxis(blocks, dim, 0)


def sum_at_owner(shard, axis, dim):
    blocks = cut_along(shard, dim, lax.axis_size(axis))
    arrived = lax.all_to_all(blocks, axis, split_axis=0, concat_axis=0, tiled=True)
    return arrived.astype(f32).sum(axis=0)


def rms_scale(values, gain):
    return values * lax.rsqrt(jnp.mean(values * values, axis=-1, keepdims=True) + eps_norm) * gain


def rotate(values, positions):
    half = values.shape[-1] // 2
    freqs = theta ** (-jnp.arange(half).astype(f32) / half)
    angles = positions[..., None] * freqs
    cosine = jnp.cos(angles)
    sine = jnp.sin(angles)
    first = values[..., :half]
    second = values[..., half:]
    return jnp.concatenate(
        [first * cosine - second * sine, second * cosine + first * sine], axis=-1
    )


def attend_kernel(
    heads, scale, xp_ref, qt_ref, ku_ref, vut_ref, out_ref,
    x, q, acc, high, acc_in, high_in,
    got, sent_a, sent_y, sent_bz, sent_by, sent_br, pair_sem,
):
    sp, tp = lax.axis_index("sp"), lax.axis_index("tp")
    core = lax.rem(sp, 2)
    y = lax.rem(sp // 2, 4)
    z = sp // 8
    rows = xp_ref.shape[1]
    own_q = qt_ref.shape[2]

    def device(pz, py):
        return (((pz * 4 + py) * 2 + core), tp)

    def turn(a, n):
        return lax.rem(a + 2 * n, n)

    up, down = device(turn(z + 1, 8), y), device(turn(z - 1, 8), y)
    right, left = device(z, turn(y + 1, 4)), device(z, turn(y - 1, 4))
    across = device(z, turn(y + 2, 4))
    sibling = (sp + 1 - 2 * core, tp)

    def slot(pz, py, color):
        return (pz * 4 + py) * 2 + color

    def send(src, at, sem, target):
        return pltpu.make_async_remote_copy(
            src_ref=src, dst_ref=x.at[at], send_sem=sem, recv_sem=got.at[at],
            device_id=target, device_id_type=pl.DeviceIdType.MESH,
        )

    def arrived(at):
        send(x.at[at], at, got.at[at], sibling).wait_recv()

    barrier = pltpu.get_barrier_semaphore()
    peers = (up, down, right, left, across, sibling)
    for peer in peers:
        pl.semaphore_signal(barrier, inc=1, device_id=peer, device_id_type=pl.DeviceIdType.MESH)
    pl.semaphore_wait(barrier, len(peers))

    own_a, own_b = slot(z, y, 0), slot(z, y, 1)
    first = [
        send(xp_ref.at[1], own_b, sent_bz.at[0, 0], up),
        send(xp_ref.at[1], own_b, sent_bz.at[0, 1], down),
        send(xp_ref.at[0], own_a, sent_y.at[0], right),
        send(xp_ref.at[0], own_a, sent_y.at[1], left),
        send(xp_ref.at[0], own_a, sent_y.at[2], across),
        send(xp_ref.at[1], own_b, sent_by.at[0, 0], right),
        send(xp_ref.at[1], own_b, sent_by.at[0, 1], left),
        send(xp_ref.at[0], own_a, sent_a.at[0, 0, 0], up),
        send(xp_ref.at[0], own_a, sent_a.at[0, 0, 1], down),
    ]
    for copy in first:
        copy.start()
    q_copy = pltpu.make_async_remote_copy(
        src_ref=qt_ref, dst_ref=q.at[1], send_sem=pair_sem.at[0], recv_sem=pair_sem.at[1],
        device_id=sibling, device_id_type=pl.DeviceIdType.MESH,
    )
    q_copy.start()
    x[own_a] = xp_ref[0]
    x[own_b] = xp_ref[1]
    q[0] = qt_ref[...]
    acc[...] = jnp.zeros_like(acc)
    high[...] = jnp.full_like(high, -jnp.inf)

    def plane(k):
        return turn(z + (1 - 2 * lax.rem(k, 2)) * ((k + 1) // 2), 8)

    def b_copies(k):
        pz = plane(k)
        at = slot(pz, y, 1)
        onward = device(turn(z + 2 * lax.rem(k, 2) - 1, 8), y)
        along = send(x.at[at], at, sent_bz.at[k, 0], onward)
        return (
            along,
            send(x.at[at], at, sent_by.at[k, 0], right),
            send(x.at[at], at, sent_by.at[k, 1], left),
        )

    def b_first(k):
        arrived(slot(plane(k), y, 1))
        along, one, two = b_copies(k)

        @pl.when(k < 6)
        def _():
            along.start()

        one.start()
        two.start()

    def relay_copy(k):
        back = (1 - lax.rem(k, 2)) * ((k + 7) // 8)
        at = slot(plane(k), turn(y - 1 + 2 * back, 4), 1)
        return send(x.at[at], at, sent_br.at[k], device(z, turn(y + 1 - 2 * back, 4)))

    def relay(k):
        arrived(slot(plane(k), turn(y - 1, 4), 1))
        arrived(slot(plane(k), turn(y + 1, 4), 1))
        relay_copy(k).start()

    def a_copy(k, j, way):
        at = slot(plane(k), turn(y + j, 4), 0)
        return send(x.at[at], at, sent_a.at[k, j, way], up if way == 0 else down)

    def a_goes(k, j, way):
        if way == 0:
            most = 5 if j < 2 else 3
            rule = jnp.logical_and(lax.rem(k, 2) == 1, k <= most)
        else:
            most = 6 if j >= 2 else 4
            rule = jnp.logical_and(lax.rem(k, 2) == 0, k <= most)
        if j == 0:
            return jnp.logical_and(rule, k > 0)
        return jnp.logical_or(rule, k == 0)

    def a_first(k):
        for j in (1, 3, 2, 0):
            at = slot(plane(k), turn(y + j, 4), 0)
            if j == 0:
                pl.when(k > 0)(functools.partial(arrived, at))
            else:
                arrived(at)
            for way in range(2):
                pl.when(a_goes(k, j, way))(a_copy(k, j, way).start)

    def compute(pz, color):
        at = [slot(pz, j, color) for j in range(4)]
        keys = rows - 16
        latent = jnp.concatenate([x[s, :keys, :] for s in at], axis=0)
        k = jnp.dot(latent, ku_ref[...], preferred_element_type=f32).astype(bf16)
        vt = lax.dot_general(
            vut_ref[...], latent, (((1,), (1,)), ((), ())), preferred_element_type=f32
        ).astype(bf16)
        even, odd = [], []
        for s in at:
            for half in range(2):
                part = x[s, keys:, 128 * half : 128 * half + 128].astype(f32)
                r1, r2, r3 = (pltpu.roll(part, 32 * n, 1) for n in (1, 2, 3))
                even += [r2, r1, part, r3]
                odd += [part, r3, r2, r1]
        even = jnp.concatenate(even, axis=0).astype(bf16)
        odd = jnp.concatenate(odd, axis=0).astype(bf16)
        lane = lax.broadcasted_iota(jnp.int32, even.shape, 1)
        count = latent.shape[0]
        ones = jnp.ones((16, count), bf16)
        vrows = vt.shape[0] // heads

        def score(h):
            pair = k[:, 128 * (h // 2) : 128 * (h // 2) + 128]
            kh = jnp.where(lane < 64, pair, even) if h % 2 == 0 else jnp.where(lane >= 64, pair, odd)
            both = jnp.concatenate([q[0, h], q[1, h]], axis=1)
            return jnp.dot(kh, both, preferred_element_type=f32)

        following = score(0)
        for h in range(heads):
            s = following
            if h + 1 < heads:
                following = score(h + 1)
            old = high[h : h + 1, :]
            new = jnp.maximum(old, jnp.max(s, axis=0, keepdims=True))
            alpha = jnp.exp2((old - new) * scale)
            p = jnp.exp2((s - new) * scale).astype(bf16)
            high[h : h + 1, :] = new
            v = jnp.concatenate([vt[h * vrows : (h + 1) * vrows], ones], axis=0)
            acc[h] = acc[h] * alpha + jnp.dot(v, p, preferred_element_type=f32)

    b_first(1)
    b_first(2)
    relay(0)
    q_copy.wait()

    @pl.loop(0, 8)
    def _(k):
        a_first(k)
        compute(plane(k), 0)
        pl.when(k < 5)(lambda: b_first(k + 3))
        pl.when(k < 7)(lambda: relay(k + 1))
        arrived(slot(plane(k), turn(y + 2, 4), 1))
        compute(plane(k), 1)

    for copy in first:
        copy.wait_send()

    @pl.loop(0, 8)
    def _(k):
        for j in range(4):
            for way in range(2):
                pl.when(a_goes(k, j, way))(a_copy(k, j, way).wait_send)
        along, one, two = b_copies(k)
        pl.when(jnp.logical_and(k > 0, k < 6))(along.wait_send)
        pl.when(k > 0)(one.wait_send)
        pl.when(k > 0)(two.wait_send)
        relay_copy(k).wait_send()

    copies = [
        pltpu.make_async_remote_copy(
            src_ref=a.at[:, own_q:] if a.ndim == 2 else a.at[:, :, own_q:],
            dst_ref=b, send_sem=pair_sem.at[2 * n + 2], recv_sem=pair_sem.at[2 * n + 3],
            device_id=sibling, device_id_type=pl.DeviceIdType.MESH,
        )
        for n, (a, b) in enumerate(((acc, acc_in), (high, high_in)))
    ]
    for copy in copies:
        copy.start()
    for copy in copies:
        copy.wait()
    vrows = vut_ref.shape[0] // heads
    for h in range(heads):
        m0, m1 = high[h : h + 1, :own_q], high_in[h : h + 1, :]
        top = jnp.maximum(m0, m1)
        a0, a1 = jnp.exp2((m0 - top) * scale), jnp.exp2((m1 - top) * scale)
        total = acc[h, vrows : vrows + 1, :own_q] * a0 + acc_in[h, vrows : vrows + 1, :] * a1
        merged = acc[h, :vrows, :own_q] * a0 + acc_in[h, :vrows, :] * a1
        out_ref[h * vrows : (h + 1) * vrows, :] = (merged / total).astype(bf16)


def attend(xp, qt, key_up, value_up_t, size):
    heads, width, own_q = qt.shape
    vdim = value_up_t.shape[0] // heads
    pieces = lax.axis_size("sp")
    vmem = pl.BlockSpec(memory_space=pltpu.VMEM)
    dma = pltpu.SemaphoreType.DMA
    scale = math.log2(math.e) * size ** (-0.5)
    return pl.pallas_call(
        functools.partial(attend_kernel, heads, scale),
        out_shape=jax.ShapeDtypeStruct((heads * vdim, own_q), bf16),
        in_specs=[vmem] * 4,
        out_specs=vmem,
        scratch_shapes=[
            pltpu.VMEM((pieces, *xp.shape[1:]), bf16),
            pltpu.VMEM((2, heads, width, own_q), bf16),
            pltpu.VMEM((heads, vdim + 16, 2 * own_q), f32),
            pltpu.VMEM((heads, 2 * own_q), f32),
            pltpu.VMEM((heads, vdim + 16, own_q), f32),
            pltpu.VMEM((heads, own_q), f32),
            dma((pieces,)),
            dma((8, 4, 2)),
            dma((3,)),
            dma((8, 2)),
            dma((8, 2)),
            dma((8,)),
            dma((6,)),
        ],
        compiler_params=pltpu.CompilerParams(
            collective_id=0, has_side_effects=True, vmem_limit_bytes=56 * 2**20
        ),
        cost_estimate=pl.CostEstimate(
            flops=2 * 128 * pieces * 2 * own_q * heads * 320,
            bytes_accessed=2 * 10**6,
            transcendentals=128 * pieces * 2 * own_q * heads,
        ),
        name="attend",
    )(xp, qt, key_up, value_up_t)


def per_device(
    tokens,
    in_gain,
    query_down,
    latent_down,
    rope_down,
    query_gain,
    latent_gain,
    query_nope,
    query_rope,
    key_up,
    value_up,
    conv_value,
    conv_gate,
    conv_taps,
    conv_bias,
    channel_gain,
    out_attend,
    out_conv,
):
    row_count = tokens.shape[0]
    width = in_gain.shape[0]
    local_ch = conv_value.shape[1]
    positions = (lax.axis_index("sp") * row_count + jnp.arange(row_count)).astype(f32)
    piece_f = gather_directly(tokens, "tp", 1).astype(f32)
    scaled = (piece_f * in_gain).astype(bf16)

    def add_rows(weight):
        return jnp.dot(scaled, weight, preferred_element_type=f32)

    square_sum = jnp.sum(piece_f * piece_f, axis=1)
    q_pre = add_rows(query_down)
    kv_pre = add_rows(latent_down)
    rope_pre = add_rows(rope_down)
    value_pre = add_rows(conv_value)
    gate_pre = add_rows(conv_gate)
    row_scale = lax.rsqrt(square_sum / width + eps_norm)[:, None]
    q_latent = rms_scale(row_scale * q_pre, query_gain).astype(bf16)
    kv_latent = rms_scale(row_scale * kv_pre, latent_gain).astype(bf16)
    rope_key = rotate(row_scale * rope_pre, positions).astype(bf16)
    rope_size = rope_down.shape[1]
    heads = query_rope.shape[1] // rope_size
    nope = query_nope.shape[1] // heads

    packed = jnp.transpose(rope_key.reshape(2, 8, 16, rope_size), (0, 2, 1, 3)).reshape(2, 16, 8 * rope_size)
    xp = jnp.concatenate([kv_latent.reshape(2, row_count // 2, -1), packed], axis=1)

    q_heads = (
        jnp.dot(q_latent, query_nope, preferred_element_type=f32)
        .astype(bf16)
        .reshape(row_count, heads, nope)
    )
    q_turn = jnp.dot(q_latent, query_rope, preferred_element_type=f32).reshape(
        row_count, heads, rope_size
    )
    r_heads = rotate(q_turn, positions[:, None]).astype(bf16)
    empty = jnp.zeros((row_count, 64 - rope_size), bf16)
    cols = []
    for h in range(heads):
        if h % 2 == 0:
            cols += [q_heads[:, h], r_heads[:, h], empty]
        else:
            cols += [r_heads[:, h], empty, q_heads[:, h]]
    q_own = jnp.transpose(jnp.concatenate(cols, axis=1))
    attended = attend(
        xp, q_own.reshape(heads, 128, row_count), key_up, jnp.transpose(value_up), nope + rope_size
    )

    glu = (row_scale * value_pre * jax.nn.sigmoid(row_scale * gate_pre)).astype(bf16)
    taps = conv_taps.shape[0]
    padded = padded_2(glu, (("sp", 0),), taps // 2).astype(f32)
    conv = jnp.zeros((row_count, local_ch), f32) + conv_bias
    for tap in range(taps):
        conv = conv + conv_taps[tap] * padded[tap : tap + row_count]
    peers = lax.axis_size("tp")
    channels = local_ch * peers
    own_mean = jnp.mean(conv, axis=-1)
    off = conv - own_mean[:, None]
    own_spread = jnp.sum(off * off, axis=-1)
    sums = sent_to_all(jnp.stack([own_mean, own_spread]), "tp")
    means = sums[:, 0]
    mean = jnp.mean(means, axis=0)
    apart = means - mean
    spread = (jnp.sum(sums[:, 1], axis=0) + local_ch * jnp.sum(apart * apart, axis=0)) / channels
    centred = conv - mean[:, None]
    activated = jax.nn.silu(
        centred * lax.rsqrt(spread[:, None] + eps_layer) * channel_gain
    ).astype(bf16)
    summed = sum_at_owner(
        (
            lax.dot_general(
                out_attend, attended, (((0,), (0,)), ((), ())), preferred_element_type=f32
            )
            + lax.dot_general(
                out_conv, activated, (((0,), (1,)), ((), ())), preferred_element_type=f32
            )
        ).astype(bf16),
        "tp",
        0,
    )
    return jnp.transpose(summed).astype(bf16)


def solution(mesh):
    in_specs = (
        P("sp", "tp"),
        P(),
        P(),
        P(),
        P(),
        P(),
        P(),
        P(None, "tp"),
        P(None, "tp"),
        P(None, "tp"),
        P(None, "tp"),
        P(None, "tp"),
        P(None, "tp"),
        P(None, "tp"),
        P("tp"),
        P("tp"),
        P("tp", None),
        P("tp", None),
    )
    return jax.shard_map(
        per_device, mesh=mesh, in_specs=in_specs, out_specs=P("sp", "tp"), check_vma=False
    )
```

```python
import functools
import math

import jax
import jax.numpy as jnp
from jax import lax
from jax.experimental import pallas as pl
from jax.experimental.pallas import tpu as pltpu
from jax.sharding import PartitionSpec as P

eps_norm = 1e-06
eps_layer = 1e-05
theta = 10000.0
bf16 = jnp.bfloat16
f32 = jnp.float32

def laid_out(blocks, dim):
    dims = list(blocks.shape[1:])
    dims[dim] *= blocks.shape[0]
    return jnp.moveaxis(blocks, 0, dim).reshape(dims)


def sent_to_all(shard, axis):
    copies = jnp.broadcast_to(shard, (lax.axis_size(axis), *shard.shape))
    return lax.all_to_all(copies, axis, split_axis=0, concat_axis=0, tiled=True)


def gather_directly(shard, axis, dim):
    return laid_out(sent_to_all(shard, axis), dim)


def padded_2(cells, sides, width):
    for axis, dim in sides:
        count = lax.axis_size(axis)
        ends = count - 1
        head = lax.slice_in_dim(cells, 0, width, axis=dim)
        tail = lax.slice_in_dim(cells, cells.shape[dim] - width, cells.shape[dim], axis=dim)
        cells = jnp.concatenate(
            [
                lax.ppermute(tail, axis, [(i, (i + 1) % count) for i in range(ends)]),
                cells,
                lax.ppermute(head, axis, [((i + 1) % count, i) for i in range(ends)]),
            ],
            axis=dim,
        )
    return cells


def cut_along(shard, dim, peers):
    dims = shard.shape
    blocks = shard.reshape(*dims[:dim], peers, dims[dim] // peers, *dims[dim + 1 :])
    return jnp.moveaxis(blocks, dim, 0)


def sum_at_owner(shard, axis, dim):
    blocks = cut_along(shard, dim, lax.axis_size(axis))
    arrived = lax.all_to_all(blocks, axis, split_axis=0, concat_axis=0, tiled=True)
    return arrived.astype(f32).sum(axis=0)


def rms_scale(values, gain):
    return values * lax.rsqrt(jnp.mean(values * values, axis=-1, keepdims=True) + eps_norm) * gain


def rotate(values, positions):
    half = values.shape[-1] // 2
    freqs = theta ** (-jnp.arange(half).astype(f32) / half)
    angles = positions[..., None] * freqs
    cosine = jnp.cos(angles)
    sine = jnp.sin(angles)
    first = values[..., :half]
    second = values[..., half:]
    return jnp.concatenate(
        [first * cosine - second * sine, second * cosine + first * sine], axis=-1
    )


def attend_kernel(
    heads, scale, xp_ref, qt_ref, ku_ref, vut_ref, out_ref,
    x, q, keys, vals, acc, high, acc_in, high_in, part_out, part_in,
    got_x, sent_x, got_q, sent_q, sent_relay, sent_pair_q, got_pair_q, pair_sem, part_sem,
):
    sp, tp = lax.axis_index("sp"), lax.axis_index("tp")
    core = lax.rem(sp, 2)
    y = lax.rem(sp // 2, 4)
    z = sp // 8
    own_q = qt_ref.shape[2]
    depth = xp_ref.shape[1] - 16
    vrows = vut_ref.shape[0] // heads
    half_heads = heads // 2

    def device(pz, py):
        return (((pz * 4 + py) * 2 + core), tp)

    def turn(a, n):
        return lax.rem(a + 2 * n, n)

    up, down = device(turn(z + 1, 8), y), device(turn(z - 1, 8), y)
    right, left = device(z, turn(y + 1, 4)), device(z, turn(y - 1, 4))
    across = device(z, turn(y + 2, 4))
    sibling = (sp + 1 - 2 * core, tp)

    def remote(src, dst, sent, got, target):
        return pltpu.make_async_remote_copy(
            src_ref=src, dst_ref=dst, send_sem=sent, recv_sem=got,
            device_id=target, device_id_type=pl.DeviceIdType.MESH,
        )

    barrier = pltpu.get_barrier_semaphore()
    peers = (up, down, right, left, across, sibling)
    for peer in peers:
        pl.semaphore_signal(barrier, inc=1, device_id=peer, device_id_type=pl.DeviceIdType.MESH)
    pl.semaphore_wait(barrier, len(peers))

    def plane(k):
        return turn(z + (1 - 2 * lax.rem(k, 2)) * ((k + 1) // 2), 8)

    def x_copy(k, n, target):
        at = x.at[plane(k), n]
        return remote(at, at, sent_x.at[k, n], got_x.at[plane(k), n], target)

    def part_of(ref, n):
        return ref.at[n * half_heads : (n + 1) * half_heads]

    def q_slot(py, who, n):
        return q.at[py, who, n * half_heads : (n + 1) * half_heads]

    first = []
    for n in range(2):
        for way, target in enumerate((up, down)):
            first.append(
                remote(xp_ref.at[n], x.at[z, n], sent_x.at[7 * way, n], got_x.at[z, n], target)
            )
    for n in range(2):
        for way, target in enumerate((right, left)):
            m = n if way == 0 else 1 - n
            first.append(
                remote(part_of(qt_ref, m), q_slot(y, core, m), sent_q.at[way, m], got_q.at[y, m], target)
            )
    for n in range(2):
        first.append(
            remote(
                part_of(qt_ref, n), q_slot(y, core, n), sent_pair_q.at[0, n],
                got_pair_q.at[y, n], sibling,
            )
        )
    for copy in first:
        copy.start()
    x[z] = xp_ref[...]
    q[y, core] = qt_ref[...]
    acc[...] = jnp.zeros_like(acc)
    high[...] = jnp.full_like(high, -jnp.inf)

    def x_next(k):
        return [
            (x_copy(k, n, up if k % 2 else down), k < 5 or (k == 5 and n == 0) or (k == 6 and n == 1))
            for n in range(2)
        ]

    def x_first(k):
        for copy, goes in x_next(k):
            copy.wait_recv()
            if goes:
                copy.start()

    def pair_q(r, n):
        py = turn(y + r, 4)
        at = q_slot(py, core, n)
        return remote(at, at, sent_pair_q.at[r, n], got_pair_q.at[py, n], sibling)

    def arrived_q(r, n):
        py = turn(y + r, 4)
        at = q_slot(py, core, n)
        remote(at, at, sent_relay.at[n], got_q.at[py, n], sibling).wait_recv()

    def relay_q(n):
        py = turn(y - 1 + 2 * n, 4)
        at = q_slot(py, core, n)
        return remote(at, at, sent_relay.at[n], got_q.at[py, n], right if n == 0 else left)

    def pair_arrived(r):
        py = turn(y + r, 4)
        for n in range(2):
            at = q_slot(py, 1 - core, n)
            remote(at, at, sent_relay.at[n], got_pair_q.at[py, n], sibling).wait_recv()

    def q_from(r, order):
        for n in order:
            arrived_q(r, n)
            if (r, n) in ((3, 0), (1, 1)):
                relay_q(n).start()
            pair_q(r, n).start()

    def swap(r):
        return [
            remote(
                acc.at[r, :, :, own_q:], acc_in.at[r], pair_sem.at[r, 0], pair_sem.at[r, 1], sibling
            ),
            remote(high.at[r, :, own_q:], high_in.at[r], pair_sem.at[r, 2], pair_sem.at[r, 3], sibling),
        ]

    def swap_start(r):
        for copy in swap(r):
            copy.start()

    def part_copy(r):
        return remote(
            part_out.at[r - 1], part_in.at[r - 1], part_sem.at[r - 1, 0], part_sem.at[r - 1, 1],
            {1: right, 2: across, 3: left}[r],
        )

    def merge(r):
        for copy in swap(r):
            copy.wait()
        for h in range(heads):
            m0, m1 = high[r, h : h + 1, :own_q], high_in[r, h : h + 1, :]
            top = jnp.maximum(m0, m1)
            a0, a1 = jnp.exp2((m0 - top) * scale), jnp.exp2((m1 - top) * scale)
            part_out[r - 1, h, :vrows, :] = (
                acc[r, h, :vrows, :own_q] * a0 + acc_in[r, h, :vrows, :] * a1
            )
            total = acc[r, h, vrows : vrows + 1, :own_q] * a0 + acc_in[r, h, vrows : vrows + 1, :] * a1
            part_out[r - 1, h, vrows:, :] = jnp.concatenate([total] * 4 + [top] * 4, axis=0)
        part_copy(r).start()

    def expand(c):
        at = [plane(2 * c), plane(2 * c + 1)]
        latent = jnp.concatenate([x[s, n, :depth, :] for s in at for n in range(2)], axis=0)
        k = jnp.dot(latent, ku_ref[...], preferred_element_type=f32).astype(bf16)
        vt = lax.dot_general(
            vut_ref[...], latent, (((1,), (1,)), ((), ())), preferred_element_type=f32
        ).astype(bf16)
        even, odd = [], []
        for s in at:
            for n in range(2):
                for half in range(2):
                    part = x[s, n, depth:, 128 * half : 128 * half + 128].astype(f32)
                    r1, r2, r3 = (pltpu.roll(part, 32 * m, 1) for m in (1, 2, 3))
                    even += [r2, r1, part, r3]
                    odd += [part, r3, r2, r1]
        even = jnp.concatenate(even, axis=0).astype(bf16)
        odd = jnp.concatenate(odd, axis=0).astype(bf16)
        lane = lax.broadcasted_iota(jnp.int32, even.shape, 1)
        for h in range(heads):
            pair = k[:, 128 * (h // 2) : 128 * (h // 2) + 128]
            keys[c, h] = (
                jnp.where(lane < 64, pair, even) if h % 2 == 0 else jnp.where(lane >= 64, pair, odd)
            )
            vals[c, h, :vrows, :] = vt[h * vrows : (h + 1) * vrows]
            vals[c, h, vrows:, :] = jnp.ones((16, vt.shape[1]), bf16)

    def compute(r, c):
        py = turn(y + r, 4)

        def score(h):
            both = jnp.concatenate([q[py, core, h], q[py, 1 - core, h]], axis=1)
            return jnp.dot(keys[c, h], both, preferred_element_type=f32)

        following = score(0)
        for h in range(heads):
            s = following
            if h + 1 < heads:
                following = score(h + 1)
            old = high[r, h : h + 1, :]
            new = jnp.maximum(old, jnp.max(s, axis=0, keepdims=True))
            alpha = jnp.exp2((old - new) * scale)
            p = jnp.exp2((s - new) * scale).astype(bf16)
            high[r, h : h + 1, :] = new
            acc[r, h] = acc[r, h] * alpha + jnp.dot(vals[c, h], p, preferred_element_type=f32)

    x_first(1)
    x_first(2)
    expand(0)
    pair_arrived(0)

    def before(step):
        if step == 1:
            x_first(3)
            x_first(4)
            q_from(1, (1, 0))
            q_from(3, (0, 1))
            pair_arrived(1)
        if step == 2:
            expand(1)
        if step == 3:
            x_first(5)
            x_first(6)
            expand(2)
        if step == 4:
            x_first(7)
            q_from(2, (0, 1))
            expand(3)
        if step == 5:
            pair_arrived(2)
            swap_start(1)
        if step == 6:
            merge(1)
        if step == 9:
            pair_arrived(3)
            swap_start(2)
        if step == 10:
            merge(2)
        if step == 13:
            swap_start(3)
        if step == 14:
            merge(3)

    @pl.loop(0, 16)
    def _(step):
        for s in (1, 2, 3, 4, 5, 6, 9, 10, 13, 14):
            pl.when(step == s)(functools.partial(before, s))
        r = lax.rem((step + 3) // 4, 4)
        c = lax.rem(step + 3, 4) + (step + 3) // 16 - 3 * (1 - (step + 15) // 16)
        compute(r, c)

    swap_start(0)
    for copy in first:
        copy.wait_send()
    for k in range(1, 8):
        for copy, goes in x_next(k):
            if goes:
                copy.wait_send()
    for n in range(2):
        relay_q(n).wait_send()
        for r in range(1, 4):
            pair_q(r, n).wait_send()
    for r in range(1, 4):
        part_copy(r).wait()
    for copy in swap(0):
        copy.wait()
    for h in range(heads):
        tops = [high[0, h : h + 1, :own_q], high_in[0, h : h + 1, :]]
        parts = [acc[0, h, : vrows + 1, :own_q], acc_in[0, h, : vrows + 1, :]]
        for r in range(3):
            tops.append(part_in[r, h, vrows + 4 : vrows + 5, :])
            parts.append(part_in[r, h, : vrows + 1, :])
        top = functools.reduce(jnp.maximum, tops)
        whole = sum(p * jnp.exp2((m - top) * scale) for p, m in zip(parts, tops))
        out_ref[h * vrows : (h + 1) * vrows, :] = (whole[:vrows] / whole[vrows : vrows + 1]).astype(bf16)


def attend(xp, qt, key_up, value_up_t, size):
    heads, width, own_q = qt.shape
    vdim = value_up_t.shape[0] // heads
    vmem = pl.BlockSpec(memory_space=pltpu.VMEM)
    dma = pltpu.SemaphoreType.DMA
    scale = math.log2(math.e) * size ** (-0.5)
    return pl.pallas_call(
        functools.partial(attend_kernel, heads, scale),
        out_shape=jax.ShapeDtypeStruct((heads * vdim, own_q), bf16),
        in_specs=[vmem] * 4,
        out_specs=vmem,
        scratch_shapes=[
            pltpu.VMEM((8, *xp.shape), bf16),
            pltpu.VMEM((4, 2, heads, width, own_q), bf16),
            pltpu.VMEM((4, heads, 2 * own_q, width), bf16),
            pltpu.VMEM((4, heads, vdim + 16, 2 * own_q), bf16),
            pltpu.VMEM((4, heads, vdim + 16, 2 * own_q), f32),
            pltpu.VMEM((4, heads, 2 * own_q), f32),
            pltpu.VMEM((4, heads, vdim + 16, own_q), f32),
            pltpu.VMEM((4, heads, own_q), f32),
            pltpu.VMEM((3, heads, vdim + 8, own_q), f32),
            pltpu.VMEM((3, heads, vdim + 8, own_q), f32),
            dma((8, 2)),
            dma((8, 2)),
            dma((4, 2)),
            dma((2, 2)),
            dma((2,)),
            dma((4, 2)),
            dma((4, 2)),
            dma((4, 4)),
            dma((3, 2)),
        ],
        compiler_params=pltpu.CompilerParams(
            collective_id=0, has_side_effects=True, vmem_limit_bytes=56 * 2**20
        ),
        cost_estimate=pl.CostEstimate(
            flops=2 * 8192 * 2 * own_q * heads * 320,
            bytes_accessed=2 * 10**6,
            transcendentals=8192 * 2 * own_q * heads,
        ),
        name="attend",
    )(xp, qt, key_up, value_up_t)


def per_device(
    tokens,
    in_gain,
    query_down,
    latent_down,
    rope_down,
    query_gain,
    latent_gain,
    query_nope,
    query_rope,
    key_up,
    value_up,
    conv_value,
    conv_gate,
    conv_taps,
    conv_bias,
    channel_gain,
    out_attend,
    out_conv,
):
    row_count = tokens.shape[0]
    width = in_gain.shape[0]
    local_ch = conv_value.shape[1]
    positions = (lax.axis_index("sp") * row_count + jnp.arange(row_count)).astype(f32)
    piece_f = gather_directly(tokens, "tp", 1).astype(f32)
    scaled = (piece_f * in_gain).astype(bf16)

    def add_rows(weight):
        return jnp.dot(scaled, weight, preferred_element_type=f32)

    square_sum = jnp.sum(piece_f * piece_f, axis=1)
    q_pre = add_rows(query_down)
    kv_pre = add_rows(latent_down)
    rope_pre = add_rows(rope_down)
    value_pre = add_rows(conv_value)
    gate_pre = add_rows(conv_gate)
    row_scale = lax.rsqrt(square_sum / width + eps_norm)[:, None]
    q_latent = rms_scale(row_scale * q_pre, query_gain).astype(bf16)
    kv_latent = rms_scale(row_scale * kv_pre, latent_gain).astype(bf16)
    rope_key = rotate(row_scale * rope_pre, positions).astype(bf16)
    rope_size = rope_down.shape[1]
    heads = query_rope.shape[1] // rope_size
    nope = query_nope.shape[1] // heads

    packed = jnp.transpose(rope_key.reshape(2, 8, 16, rope_size), (0, 2, 1, 3)).reshape(2, 16, 8 * rope_size)
    xp = jnp.concatenate([kv_latent.reshape(2, row_count // 2, -1), packed], axis=1)

    q_heads = (
        jnp.dot(q_latent, query_nope, preferred_element_type=f32)
        .astype(bf16)
        .reshape(row_count, heads, nope)
    )
    q_turn = jnp.dot(q_latent, query_rope, preferred_element_type=f32).reshape(
        row_count, heads, rope_size
    )
    r_heads = rotate(q_turn, positions[:, None]).astype(bf16)
    empty = jnp.zeros((row_count, 64 - rope_size), bf16)
    cols = []
    for h in range(heads):
        if h % 2 == 0:
            cols += [q_heads[:, h], r_heads[:, h], empty]
        else:
            cols += [r_heads[:, h], empty, q_heads[:, h]]
    q_own = jnp.transpose(jnp.concatenate(cols, axis=1))
    attended = attend(
        xp, q_own.reshape(heads, 128, row_count), key_up, jnp.transpose(value_up), nope + rope_size
    )

    glu = (row_scale * value_pre * jax.nn.sigmoid(row_scale * gate_pre)).astype(bf16)
    taps = conv_taps.shape[0]
    padded = padded_2(glu, (("sp", 0),), taps // 2).astype(f32)
    conv = jnp.zeros((row_count, local_ch), f32) + conv_bias
    for tap in range(taps):
        conv = conv + conv_taps[tap] * padded[tap : tap + row_count]
    peers = lax.axis_size("tp")
    channels = local_ch * peers
    own_mean = jnp.mean(conv, axis=-1)
    off = conv - own_mean[:, None]
    own_spread = jnp.sum(off * off, axis=-1)
    sums = sent_to_all(jnp.stack([own_mean, own_spread]), "tp")
    means = sums[:, 0]
    mean = jnp.mean(means, axis=0)
    apart = means - mean
    spread = (jnp.sum(sums[:, 1], axis=0) + local_ch * jnp.sum(apart * apart, axis=0)) / channels
    centred = conv - mean[:, None]
    activated = jax.nn.silu(
        centred * lax.rsqrt(spread[:, None] + eps_layer) * channel_gain
    ).astype(bf16)
    summed = sum_at_owner(
        (
            lax.dot_general(
                out_attend, attended, (((0,), (0,)), ((), ())), preferred_element_type=f32
            )
            + lax.dot_general(
                out_conv, activated, (((0,), (1,)), ((), ())), preferred_element_type=f32
            )
        ).astype(bf16),
        "tp",
        0,
    )
    return jnp.transpose(summed).astype(bf16)


def solution(mesh):
    in_specs = (
        P("sp", "tp"),
        P(),
        P(),
        P(),
        P(),
        P(),
        P(),
        P(None, "tp"),
        P(None, "tp"),
        P(None, "tp"),
        P(None, "tp"),
        P(None, "tp"),
        P(None, "tp"),
        P(None, "tp"),
        P("tp"),
        P("tp"),
        P("tp", None),
        P("tp", None),
    )
    return jax.shard_map(
        per_device, mesh=mesh, in_specs=in_specs, out_specs=P("sp", "tp"), check_vma=False
    )
```

```python
import functools
import math

import jax
import jax.numpy as jnp
from jax import lax
from jax.experimental import pallas as pl
from jax.experimental.pallas import tpu as pltpu
from jax.sharding import PartitionSpec as P

eps_norm = 1e-06
eps_layer = 1e-05
theta = 10000.0
bf16 = jnp.bfloat16
f32 = jnp.float32

def laid_out(blocks, dim):
    dims = list(blocks.shape[1:])
    dims[dim] *= blocks.shape[0]
    return jnp.moveaxis(blocks, 0, dim).reshape(dims)


def sent_to_all(shard, axis):
    copies = jnp.broadcast_to(shard, (lax.axis_size(axis), *shard.shape))
    return lax.all_to_all(copies, axis, split_axis=0, concat_axis=0, tiled=True)


def gather_directly(shard, axis, dim):
    return laid_out(sent_to_all(shard, axis), dim)


def padded_2(cells, sides, width):
    for axis, dim in sides:
        count = lax.axis_size(axis)
        ends = count - 1
        head = lax.slice_in_dim(cells, 0, width, axis=dim)
        tail = lax.slice_in_dim(cells, cells.shape[dim] - width, cells.shape[dim], axis=dim)
        cells = jnp.concatenate(
            [
                lax.ppermute(tail, axis, [(i, (i + 1) % count) for i in range(ends)]),
                cells,
                lax.ppermute(head, axis, [((i + 1) % count, i) for i in range(ends)]),
            ],
            axis=dim,
        )
    return cells


def rms_scale(values, gain):
    return values * lax.rsqrt(jnp.mean(values * values, axis=-1, keepdims=True) + eps_norm) * gain


def rotate(values, positions):
    half = values.shape[-1] // 2
    freqs = theta ** (-jnp.arange(half).astype(f32) / half)
    angles = positions[..., None] * freqs
    cosine = jnp.cos(angles)
    sine = jnp.sin(angles)
    first = values[..., :half]
    second = values[..., half:]
    return jnp.concatenate(
        [first * cosine - second * sine, second * cosine + first * sine], axis=-1
    )


def attend_kernel(
    heads, scale, xp_ref, qt_ref, ku_ref, vut_ref, wa_ref, cp_ref, out_ref,
    x, q, keys, vals, acc, high, acc_in, high_in, part_out, stat_out, part_in, stat_in, wide, conv_in, weight_in,
    got_x, sent_x, got_q, sent_q, sent_relay, sent_pair_q, got_pair_q, pair_sem, part_sem,
    sent_t, got_t,
):
    sp, tp = lax.axis_index("sp"), lax.axis_index("tp")
    core = lax.rem(sp, 2)
    y = lax.rem(sp // 2, 4)
    z = sp // 8
    own_q = qt_ref.shape[2]
    depth = xp_ref.shape[1] - 16
    vrows = vut_ref.shape[0] // heads
    half_heads = heads // 2

    def device(pz, py):
        return (((pz * 4 + py) * 2 + core), tp)

    def turn(a, n):
        return lax.rem(a + 2 * n, n)

    up, down = device(turn(z + 1, 8), y), device(turn(z - 1, 8), y)
    right, left = device(z, turn(y + 1, 4)), device(z, turn(y - 1, 4))
    across = device(z, turn(y + 2, 4))
    sibling = (sp + 1 - 2 * core, tp)

    def remote(src, dst, sent, got, target):
        return pltpu.make_async_remote_copy(
            src_ref=src, dst_ref=dst, send_sem=sent, recv_sem=got,
            device_id=target, device_id_type=pl.DeviceIdType.MESH,
        )

    barrier = pltpu.get_barrier_semaphore()
    others = [(sp, lax.rem(tp + i, 4)) for i in (1, 3, 2)]
    peers = (up, down, right, left, across, sibling, *others)
    for peer in peers:
        pl.semaphore_signal(barrier, inc=1, device_id=peer, device_id_type=pl.DeviceIdType.MESH)
    pl.semaphore_wait(barrier, len(peers))

    def plane(k):
        return turn(z + (1 - 2 * lax.rem(k, 2)) * ((k + 1) // 2), 8)

    def x_copy(k, n, target):
        at = x.at[plane(k), n]
        return remote(at, at, sent_x.at[k, n], got_x.at[plane(k), n], target)

    def part_of(ref, n):
        return ref.at[n * half_heads : (n + 1) * half_heads]

    def q_slot(py, who, n):
        return q.at[py, who, n * half_heads : (n + 1) * half_heads]

    first = []
    for n in range(2):
        for way, target in enumerate((up, down)):
            first.append(
                remote(xp_ref.at[n], x.at[z, n], sent_x.at[7 * way, n], got_x.at[z, n], target)
            )
    for n in range(2):
        for way, target in enumerate((right, left)):
            m = n if way == 0 else 1 - n
            first.append(
                remote(part_of(qt_ref, m), q_slot(y, core, m), sent_q.at[way, m], got_q.at[y, m], target)
            )
    for n in range(2):
        first.append(
            remote(
                part_of(qt_ref, n), q_slot(y, core, n), sent_pair_q.at[0, n],
                got_pair_q.at[y, n], sibling,
            )
        )
    columns = out_ref.shape[1]

    def block(ref, n):
        return ref.at[:, pl.ds(pl.multiple_of(n * columns, columns), columns)]

    for i, peer in enumerate(others):
        for kind, (src, dst) in enumerate(((wa_ref, weight_in), (cp_ref, conv_in))):
            first.append(
                remote(block(src, peer[1]), dst.at[tp], sent_t.at[kind, i], got_t.at[kind, tp], peer)
            )
    for copy in first:
        copy.start()
    x[z] = xp_ref[...]
    q[y, core] = qt_ref[...]
    acc[...] = jnp.zeros_like(acc)
    high[...] = jnp.full_like(high, -jnp.inf)

    def goes(k, n):
        return k < 5 or (k == 5 and n == 0) or (k == 6 and n == 1)

    def x_first(k):
        for n in range(2):
            copy = x_copy(k, n, up if k % 2 else down)
            copy.wait_recv()
            if goes(k, n):
                copy.start()

    def pair_q(r, n):
        py = turn(y + r, 4)
        at = q_slot(py, core, n)
        return remote(at, at, sent_pair_q.at[r, n], got_pair_q.at[py, n], sibling)

    def arrived_q(r, n):
        py = turn(y + r, 4)
        at = q_slot(py, core, n)
        remote(at, at, sent_relay.at[n], got_q.at[py, n], sibling).wait_recv()

    def relay_q(n):
        py = turn(y - 1 + 2 * n, 4)
        at = q_slot(py, core, n)
        return remote(at, at, sent_relay.at[n], got_q.at[py, n], right if n == 0 else left)

    def pair_arrived(r):
        py = turn(y + r, 4)
        for n in range(2):
            at = q_slot(py, 1 - core, n)
            remote(at, at, sent_relay.at[n], got_pair_q.at[py, n], sibling).wait_recv()

    def q_from(r, order):
        for n in order:
            arrived_q(r, n)
            if (r, n) in ((3, 0), (1, 1)):
                relay_q(n).start()
            pair_q(r, n).start()

    def swap(r):
        return [
            remote(
                acc.at[r, :, :, own_q:], acc_in.at[r], pair_sem.at[r, 0], pair_sem.at[r, 1], sibling
            ),
            remote(high.at[r, :, own_q:], high_in.at[r], pair_sem.at[r, 2], pair_sem.at[r, 3], sibling),
        ]

    def swap_start(r):
        for copy in swap(r):
            copy.start()

    def part_copy(r):
        return [
            remote(
                out.at[r - 1], into.at[r - 1], part_sem.at[r - 1, n, 0], part_sem.at[r - 1, n, 1],
                {1: right, 2: across, 3: left}[r],
            )
            for n, (out, into) in enumerate(((stat_out, stat_in), (part_out, part_in)))
        ]

    def merge(r):
        for copy in swap(r):
            copy.wait()
        for h in range(heads):
            m0, m1 = high[r, h : h + 1, :own_q], high_in[r, h : h + 1, :]
            top = jnp.maximum(m0, m1)
            a0, a1 = jnp.exp2((m0 - top) * scale), jnp.exp2((m1 - top) * scale)
            total = acc[r, h, vrows : vrows + 1, :own_q] * a0 + acc_in[r, h, vrows : vrows + 1, :] * a1
            whole = acc[r, h, :vrows, :own_q] * a0 + acc_in[r, h, :vrows, :] * a1
            part_out[r - 1, h] = (whole / total).astype(bf16)
            stat_out[r - 1, h] = jnp.concatenate([total] * 4 + [top] * 4, axis=0)
        for copy in part_copy(r):
            copy.start()

    def expand(c):
        at = [plane(2 * c), plane(2 * c + 1)]
        latent = jnp.concatenate([x[s, n, :depth, :] for s in at for n in range(2)], axis=0)
        k = jnp.dot(latent, ku_ref[...], preferred_element_type=f32).astype(bf16)
        vt = lax.dot_general(
            vut_ref[...], latent, (((1,), (1,)), ((), ())), preferred_element_type=f32
        ).astype(bf16)
        even, odd = [], []
        for s in at:
            for n in range(2):
                for half in range(2):
                    part = x[s, n, depth:, 128 * half : 128 * half + 128].astype(f32)
                    r1, r2, r3 = (pltpu.roll(part, 32 * m, 1) for m in (1, 2, 3))
                    even += [r2, r1, part, r3]
                    odd += [part, r3, r2, r1]
        even = jnp.concatenate(even, axis=0).astype(bf16)
        odd = jnp.concatenate(odd, axis=0).astype(bf16)
        lane = lax.broadcasted_iota(jnp.int32, even.shape, 1)
        for h in range(heads):
            pair = k[:, 128 * (h // 2) : 128 * (h // 2) + 128]
            keys[c, h] = (
                jnp.where(lane < 64, pair, even) if h % 2 == 0 else jnp.where(lane >= 64, pair, odd)
            )
            vals[c, h, :vrows, :] = vt[h * vrows : (h + 1) * vrows]
            vals[c, h, vrows:, :] = jnp.ones((16, vt.shape[1]), bf16)

    def compute(r, c):
        py = turn(y + r, 4)

        def score(h):
            both = jnp.concatenate([q[py, core, h], q[py, 1 - core, h]], axis=1)
            return jnp.dot(keys[c, h], both, preferred_element_type=f32)

        following = score(0)
        for h in range(heads):
            s = following
            if h + 1 < heads:
                following = score(h + 1)
            old = high[r, h : h + 1, :]
            new = jnp.maximum(old, jnp.max(s, axis=0, keepdims=True))
            alpha = jnp.exp2((old - new) * scale)
            p = jnp.exp2((s - new) * scale).astype(bf16)
            high[r, h : h + 1, :] = new
            acc[r, h] = acc[r, h] * alpha + jnp.dot(vals[c, h], p, preferred_element_type=f32)

    x_first(1)
    x_first(2)
    expand(0)
    pair_arrived(0)

    def before(step):
        if step == 1:
            x_first(3)
            x_first(4)
            q_from(1, (1, 0))
            q_from(3, (0, 1))
            pair_arrived(1)
        if step == 2:
            expand(1)
        if step == 3:
            x_first(5)
            x_first(6)
            expand(2)
        if step == 4:
            x_first(7)
            q_from(2, (0, 1))
            expand(3)
        if step == 5:
            pair_arrived(2)
            swap_start(1)
        if step == 6:
            merge(1)
        if step == 9:
            pair_arrived(3)
            swap_start(2)
        if step == 10:
            merge(2)
        if step == 13:
            swap_start(3)
        if step == 14:
            merge(3)

    @pl.loop(0, 16)
    def _(step):
        for s in (1, 2, 3, 4, 5, 6, 9, 10, 13, 14):
            pl.when(step == s)(functools.partial(before, s))
        r = lax.rem((step + 3) // 4, 4)
        c = lax.rem(step + 3, 4) + (step + 3) // 16 - 3 * (1 - (step + 15) // 16)
        compute(r, c)

    swap_start(0)
    for copy in first:
        copy.wait_send()
    for k in range(1, 8):
        for n in range(2):
            if goes(k, n):
                x_copy(k, n, up if k % 2 else down).wait_send()
    for n in range(2):
        relay_q(n).wait_send()
        for r in range(1, 4):
            pair_q(r, n).wait_send()
    for r in range(1, 4):
        for copy in part_copy(r):
            copy.wait()
    for copy in swap(0):
        copy.wait()
    for h in range(heads):
        tops = [high[0, h : h + 1, :own_q], high_in[0, h : h + 1, :]]
        totals = [acc[0, h, vrows : vrows + 1, :own_q], acc_in[0, h, vrows : vrows + 1, :]]
        for r in range(3):
            tops.append(stat_in[r, h, 4:5, :])
            totals.append(stat_in[r, h, 0:1, :])
        top = functools.reduce(jnp.maximum, tops)
        shares = [jnp.exp2((m - top) * scale) for m in tops]
        total = sum(t * a for t, a in zip(totals, shares))
        whole = acc[0, h, :vrows, :own_q] * shares[0] + acc_in[0, h, :vrows, :] * shares[1]
        for r in range(3):
            whole = whole + part_in[r, h].astype(f32) * (shares[2 + r] * totals[2 + r])
        wide[tp, :, h * vrows : (h + 1) * vrows] = jnp.transpose(whole / total).astype(bf16)
    last = [
        remote(wide.at[tp], wide.at[tp], sent_t.at[2, i], got_t.at[2, tp], peer)
        for i, peer in enumerate(others)
    ]
    for copy in last:
        copy.start()
    result = jnp.dot(wide[tp], block(wa_ref, tp)[...], preferred_element_type=f32)
    result = result + block(cp_ref, tp)[...].astype(f32)
    for i in (1, 3, 2):
        source = lax.rem(tp + i, 4)
        for kind, dst in enumerate((weight_in, conv_in, wide)):
            at = dst.at[source]
            remote(at, at, sent_t.at[kind, 0], got_t.at[kind, source], others[0]).wait_recv()
        result = result + jnp.dot(wide[source], weight_in[source], preferred_element_type=f32)
        result = result + conv_in[source].astype(f32)
    out_ref[...] = result.astype(bf16)
    for copy in last:
        copy.wait_send()


def attend(xp, qt, key_up, value_up_t, out_attend, conv_part, size):
    heads, width, own_q = qt.shape
    vdim = value_up_t.shape[0] // heads
    columns = out_attend.shape[1] // 4
    vmem = pl.BlockSpec(memory_space=pltpu.VMEM)
    dma = pltpu.SemaphoreType.DMA
    scale = math.log2(math.e) * size ** (-0.5)
    return pl.pallas_call(
        functools.partial(attend_kernel, heads, scale),
        out_shape=jax.ShapeDtypeStruct((own_q, columns), bf16),
        in_specs=[vmem] * 6,
        out_specs=vmem,
        scratch_shapes=[
            pltpu.VMEM((8, *xp.shape), bf16),
            pltpu.VMEM((4, 2, heads, width, own_q), bf16),
            pltpu.VMEM((4, heads, 2 * own_q, width), bf16),
            pltpu.VMEM((4, heads, vdim + 16, 2 * own_q), bf16),
            pltpu.VMEM((4, heads, vdim + 16, 2 * own_q), f32),
            pltpu.VMEM((4, heads, 2 * own_q), f32),
            pltpu.VMEM((4, heads, vdim + 16, own_q), f32),
            pltpu.VMEM((4, heads, own_q), f32),
            pltpu.VMEM((3, heads, vdim, own_q), bf16),
            pltpu.VMEM((3, heads, 8, own_q), f32),
            pltpu.VMEM((3, heads, vdim, own_q), bf16),
            pltpu.VMEM((3, heads, 8, own_q), f32),
            pltpu.VMEM((4, own_q, heads * vdim), bf16),
            pltpu.VMEM((4, own_q, columns), bf16),
            pltpu.VMEM((4, heads * vdim, columns), bf16),
            dma((8, 2)),
            dma((8, 2)),
            dma((4, 2)),
            dma((2, 2)),
            dma((2,)),
            dma((4, 2)),
            dma((4, 2)),
            dma((4, 4)),
            dma((3, 2, 2)),
            dma((3, 3)),
            dma((3, 4)),
        ],
        compiler_params=pltpu.CompilerParams(
            collective_id=0, has_side_effects=True, vmem_limit_bytes=56 * 2**20
        ),
        cost_estimate=pl.CostEstimate(
            flops=2 * 8192 * 2 * own_q * heads * 320,
            bytes_accessed=2 * 10**6,
            transcendentals=8192 * 2 * own_q * heads,
        ),
        name="attend",
    )(xp, qt, key_up, value_up_t, out_attend, conv_part)


def per_device(
    tokens,
    in_gain,
    query_down,
    latent_down,
    rope_down,
    query_gain,
    latent_gain,
    query_nope,
    query_rope,
    key_up,
    value_up,
    conv_value,
    conv_gate,
    conv_taps,
    conv_bias,
    channel_gain,
    out_attend,
    out_conv,
):
    row_count = tokens.shape[0]
    width = in_gain.shape[0]
    local_ch = conv_value.shape[1]
    positions = (lax.axis_index("sp") * row_count + jnp.arange(row_count)).astype(f32)
    piece_f = gather_directly(tokens, "tp", 1).astype(f32)
    scaled = (piece_f * in_gain).astype(bf16)

    def add_rows(weight):
        return jnp.dot(scaled, weight, preferred_element_type=f32)

    square_sum = jnp.sum(piece_f * piece_f, axis=1)
    q_pre = add_rows(query_down)
    kv_pre = add_rows(latent_down)
    rope_pre = add_rows(rope_down)
    value_pre = add_rows(conv_value)
    gate_pre = add_rows(conv_gate)
    row_scale = lax.rsqrt(square_sum / width + eps_norm)[:, None]
    q_latent = rms_scale(row_scale * q_pre, query_gain).astype(bf16)
    kv_latent = rms_scale(row_scale * kv_pre, latent_gain).astype(bf16)
    rope_key = rotate(row_scale * rope_pre, positions).astype(bf16)
    rope_size = rope_down.shape[1]
    heads = query_rope.shape[1] // rope_size
    nope = query_nope.shape[1] // heads

    packed = jnp.transpose(rope_key.reshape(2, 8, 16, rope_size), (0, 2, 1, 3)).reshape(2, 16, 8 * rope_size)
    xp = jnp.concatenate([kv_latent.reshape(2, row_count // 2, -1), packed], axis=1)

    q_heads = (
        jnp.dot(q_latent, query_nope, preferred_element_type=f32)
        .astype(bf16)
        .reshape(row_count, heads, nope)
    )
    q_turn = jnp.dot(q_latent, query_rope, preferred_element_type=f32).reshape(
        row_count, heads, rope_size
    )
    r_heads = rotate(q_turn, positions[:, None]).astype(bf16)
    empty = jnp.zeros((row_count, 64 - rope_size), bf16)
    cols = []
    for h in range(heads):
        if h % 2 == 0:
            cols += [q_heads[:, h], r_heads[:, h], empty]
        else:
            cols += [r_heads[:, h], empty, q_heads[:, h]]
    q_own = jnp.transpose(jnp.concatenate(cols, axis=1))
    glu = (row_scale * value_pre * jax.nn.sigmoid(row_scale * gate_pre)).astype(bf16)
    taps = conv_taps.shape[0]
    padded = padded_2(glu, (("sp", 0),), taps // 2).astype(f32)
    conv = jnp.zeros((row_count, local_ch), f32) + conv_bias
    for tap in range(taps):
        conv = conv + conv_taps[tap] * padded[tap : tap + row_count]
    peers = lax.axis_size("tp")
    channels = local_ch * peers
    own_mean = jnp.mean(conv, axis=-1)
    off = conv - own_mean[:, None]
    own_spread = jnp.sum(off * off, axis=-1)
    sums = sent_to_all(jnp.stack([own_mean, own_spread]), "tp")
    means = sums[:, 0]
    mean = jnp.mean(means, axis=0)
    apart = means - mean
    spread = (jnp.sum(sums[:, 1], axis=0) + local_ch * jnp.sum(apart * apart, axis=0)) / channels
    centred = conv - mean[:, None]
    activated = jax.nn.silu(
        centred * lax.rsqrt(spread[:, None] + eps_layer) * channel_gain
    ).astype(bf16)
    conv_part = jnp.dot(activated, out_conv, preferred_element_type=f32).astype(bf16)
    return attend(
        xp,
        q_own.reshape(heads, 128, row_count),
        key_up,
        jnp.transpose(value_up),
        out_attend,
        conv_part,
        nope + rope_size,
    )


def solution(mesh):
    in_specs = (
        P("sp", "tp"),
        P(),
        P(),
        P(),
        P(),
        P(),
        P(),
        P(None, "tp"),
        P(None, "tp"),
        P(None, "tp"),
        P(None, "tp"),
        P(None, "tp"),
        P(None, "tp"),
        P(None, "tp"),
        P("tp"),
        P("tp"),
        P("tp", None),
        P("tp", None),
    )
    return jax.shard_map(
        per_device, mesh=mesh, in_specs=in_specs, out_specs=P("sp", "tp"), check_vma=False
    )
```

```python
import functools
import math

import jax
import jax.numpy as jnp
from jax import lax
from jax.experimental import pallas as pl
from jax.experimental.pallas import tpu as pltpu
from jax.sharding import PartitionSpec as P

eps_norm = 1e-06
eps_layer = 1e-05
theta = 10000.0
bf16 = jnp.bfloat16
f32 = jnp.float32

def laid_out(blocks, dim):
    dims = list(blocks.shape[1:])
    dims[dim] *= blocks.shape[0]
    return jnp.moveaxis(blocks, 0, dim).reshape(dims)


def sent_to_all(shard, axis):
    copies = jnp.broadcast_to(shard, (lax.axis_size(axis), *shard.shape))
    return lax.all_to_all(copies, axis, split_axis=0, concat_axis=0, tiled=True)


def gather_directly(shard, axis, dim):
    return laid_out(sent_to_all(shard, axis), dim)


def rms_scale(values, gain):
    return values * lax.rsqrt(jnp.mean(values * values, axis=-1, keepdims=True) + eps_norm) * gain


def rotate(values, positions):
    half = values.shape[-1] // 2
    freqs = theta ** (-jnp.arange(half).astype(f32) / half)
    angles = positions[..., None] * freqs
    cosine = jnp.cos(angles)
    sine = jnp.sin(angles)
    first = values[..., :half]
    second = values[..., half:]
    return jnp.concatenate(
        [first * cosine - second * sine, second * cosine + first * sine], axis=-1
    )


def attend_kernel(
    heads, scale, xp_ref, qt_ref, ku_ref, vut_ref, wa_ref, glu_ref,
    taps_ref, bias_ref, gain_ref, oc_ref, out_ref,
    x, q, keys, vals, acc, high, acc_in, high_in, part_out, stat_out, part_in, stat_in, wide, conv_in, weight_in,
    halo, padded, shifted, conv, moments, active, cp_ref,
    got_x, sent_x, got_q, sent_q, sent_relay, sent_pair_q, got_pair_q, pair_sem, part_sem,
    sent_t, got_t, halo_sem, sent_m, got_m,
):
    sp, tp = lax.axis_index("sp"), lax.axis_index("tp")
    core = lax.rem(sp, 2)
    y = lax.rem(sp // 2, 4)
    z = sp // 8
    own_q = qt_ref.shape[2]
    depth = xp_ref.shape[1] - 16
    vrows = vut_ref.shape[0] // heads
    half_heads = heads // 2

    def device(pz, py):
        return (((pz * 4 + py) * 2 + core), tp)

    def turn(a, n):
        return lax.rem(a + 2 * n, n)

    up, down = device(turn(z + 1, 8), y), device(turn(z - 1, 8), y)
    right, left = device(z, turn(y + 1, 4)), device(z, turn(y - 1, 4))
    across = device(z, turn(y + 2, 4))
    sibling = (sp + 1 - 2 * core, tp)

    def remote(src, dst, sent, got, target):
        return pltpu.make_async_remote_copy(
            src_ref=src, dst_ref=dst, send_sem=sent, recv_sem=got,
            device_id=target, device_id_type=pl.DeviceIdType.MESH,
        )

    barrier = pltpu.get_barrier_semaphore()
    others = [(sp, lax.rem(tp + i, 4)) for i in (1, 3, 2)]
    count = 64
    beside = [(lax.rem(sp + 1, count), tp), (lax.rem(sp + count - 1, count), tp)]
    peers = (up, down, right, left, across, sibling, *others, *beside)
    for peer in peers:
        pl.semaphore_signal(barrier, inc=1, device_id=peer, device_id_type=pl.DeviceIdType.MESH)
    pl.semaphore_wait(barrier, len(peers))

    def plane(k):
        return turn(z + (1 - 2 * lax.rem(k, 2)) * ((k + 1) // 2), 8)

    def x_copy(k, n, target):
        at = x.at[plane(k), n]
        return remote(at, at, sent_x.at[k, n], got_x.at[plane(k), n], target)

    def part_of(ref, n):
        return ref.at[n * half_heads : (n + 1) * half_heads]

    def q_slot(py, who, n):
        return q.at[py, who, n * half_heads : (n + 1) * half_heads]

    first = []
    for n in range(2):
        for way, target in enumerate((up, down)):
            first.append(
                remote(xp_ref.at[n], x.at[z, n], sent_x.at[7 * way, n], got_x.at[z, n], target)
            )
    for n in range(2):
        for way, target in enumerate((right, left)):
            m = n if way == 0 else 1 - n
            first.append(
                remote(part_of(qt_ref, m), q_slot(y, core, m), sent_q.at[way, m], got_q.at[y, m], target)
            )
    for n in range(2):
        first.append(
            remote(
                part_of(qt_ref, n), q_slot(y, core, n), sent_pair_q.at[0, n],
                got_pair_q.at[y, n], sibling,
            )
        )
    columns = out_ref.shape[1]

    def block(ref, n):
        return ref.at[:, pl.ds(pl.multiple_of(n * columns, columns), columns)]

    def block_copy(kind, i, src, dst):
        peer = others[i]
        return remote(block(src, peer[1]), dst.at[tp], sent_t.at[kind, i], got_t.at[kind, tp], peer)

    halos = [
        remote(
            glu_ref.at[own_q - 16 :] if n == 0 else glu_ref.at[:16],
            halo.at[n], halo_sem.at[n, 0], halo_sem.at[n, 1], beside[n],
        )
        for n in range(2)
    ]
    first = halos + first + [block_copy(0, i, wa_ref, weight_in) for i in range(3)]
    for copy in first:
        copy.start()
    x[z] = xp_ref[...]
    q[y, core] = qt_ref[...]
    acc[...] = jnp.zeros_like(acc)
    high[...] = jnp.full_like(high, -jnp.inf)

    def goes(k, n):
        return k < 5 or (k == 5 and n == 0) or (k == 6 and n == 1)

    def x_first(k):
        for n in range(2):
            copy = x_copy(k, n, up if k % 2 else down)
            copy.wait_recv()
            if goes(k, n):
                copy.start()

    def pair_q(r, n):
        py = turn(y + r, 4)
        at = q_slot(py, core, n)
        return remote(at, at, sent_pair_q.at[r, n], got_pair_q.at[py, n], sibling)

    def arrived_q(r, n):
        py = turn(y + r, 4)
        at = q_slot(py, core, n)
        remote(at, at, sent_relay.at[n], got_q.at[py, n], sibling).wait_recv()

    def relay_q(n):
        py = turn(y - 1 + 2 * n, 4)
        at = q_slot(py, core, n)
        return remote(at, at, sent_relay.at[n], got_q.at[py, n], right if n == 0 else left)

    def pair_arrived(r):
        py = turn(y + r, 4)
        for n in range(2):
            at = q_slot(py, 1 - core, n)
            remote(at, at, sent_relay.at[n], got_pair_q.at[py, n], sibling).wait_recv()

    def q_from(r, order):
        for n in order:
            arrived_q(r, n)
            if (r, n) in ((3, 0), (1, 1)):
                relay_q(n).start()
            pair_q(r, n).start()

    def swap(r):
        return [
            remote(
                acc.at[r, :, :, own_q:], acc_in.at[r], pair_sem.at[r, 0], pair_sem.at[r, 1], sibling
            ),
            remote(high.at[r, :, own_q:], high_in.at[r], pair_sem.at[r, 2], pair_sem.at[r, 3], sibling),
        ]

    def swap_start(r):
        for copy in swap(r):
            copy.start()

    def part_copy(r):
        return [
            remote(
                out.at[r - 1], into.at[r - 1], part_sem.at[r - 1, n, 0], part_sem.at[r - 1, n, 1],
                {1: right, 2: across, 3: left}[r],
            )
            for n, (out, into) in enumerate(((stat_out, stat_in), (part_out, part_in)))
        ]

    def merge(r):
        for copy in swap(r):
            copy.wait()
        for h in range(heads):
            m0, m1 = high[r, h : h + 1, :own_q], high_in[r, h : h + 1, :]
            top = jnp.maximum(m0, m1)
            a0, a1 = jnp.exp2((m0 - top) * scale), jnp.exp2((m1 - top) * scale)
            total = acc[r, h, vrows : vrows + 1, :own_q] * a0 + acc_in[r, h, vrows : vrows + 1, :] * a1
            whole = acc[r, h, :vrows, :own_q] * a0 + acc_in[r, h, :vrows, :] * a1
            part_out[r - 1, h] = (whole / total).astype(bf16)
            stat_out[r - 1, h] = jnp.concatenate([total] * 4 + [top] * 4, axis=0)
        for copy in part_copy(r):
            copy.start()

    def expand(c):
        at = [plane(2 * c), plane(2 * c + 1)]
        latent = jnp.concatenate([x[s, n, :depth, :] for s in at for n in range(2)], axis=0)
        k = jnp.dot(latent, ku_ref[...], preferred_element_type=f32).astype(bf16)
        vt = lax.dot_general(
            vut_ref[...], latent, (((1,), (1,)), ((), ())), preferred_element_type=f32
        ).astype(bf16)
        even, odd = [], []
        for s in at:
            for n in range(2):
                for half in range(2):
                    part = x[s, n, depth:, 128 * half : 128 * half + 128].astype(f32)
                    r1, r2, r3 = (pltpu.roll(part, 32 * m, 1) for m in (1, 2, 3))
                    even += [r2, r1, part, r3]
                    odd += [part, r3, r2, r1]
        even = jnp.concatenate(even, axis=0).astype(bf16)
        odd = jnp.concatenate(odd, axis=0).astype(bf16)
        lane = lax.broadcasted_iota(jnp.int32, even.shape, 1)
        for h in range(heads):
            pair = k[:, 128 * (h // 2) : 128 * (h // 2) + 128]
            keys[c, h] = (
                jnp.where(lane < 64, pair, even) if h % 2 == 0 else jnp.where(lane >= 64, pair, odd)
            )
            vals[c, h, :vrows, :] = vt[h * vrows : (h + 1) * vrows]
            vals[c, h, vrows:, :] = jnp.ones((16, vt.shape[1]), bf16)

    def compute(r, c):
        py = turn(y + r, 4)

        def score(h):
            both = jnp.concatenate([q[py, core, h], q[py, 1 - core, h]], axis=1)
            return jnp.dot(keys[c, h], both, preferred_element_type=f32)

        following = score(0)
        for h in range(heads):
            s = following
            if h + 1 < heads:
                following = score(h + 1)
            old = high[r, h : h + 1, :]
            new = jnp.maximum(old, jnp.max(s, axis=0, keepdims=True))
            alpha = jnp.exp2((old - new) * scale)
            p = jnp.exp2((s - new) * scale).astype(bf16)
            high[r, h : h + 1, :] = new
            acc[r, h] = acc[r, h] * alpha + jnp.dot(vals[c, h], p, preferred_element_type=f32)

    channels = glu_ref.shape[1]

    def convolve():
        for copy in halos:
            copy.wait_recv()
        padded[16 : 16 + own_q, :] = glu_ref[...].astype(f32)
        padded[:16, :] = jnp.where(sp > 0, halo[0].astype(f32), 0.0)
        padded[16 + own_q :, :] = jnp.where(sp < count - 1, halo[1].astype(f32), 0.0)
        taps = taps_ref.shape[0]
        for at in range(0, channels, 128):
            lanes = slice(at, at + 128)
            total = jnp.broadcast_to(bias_ref[:, lanes], (own_q, 128))
            for r in range(8):
                part = None
                for j in range(4):
                    k = 8 * j + r - 1
                    if 0 <= k < taps:
                        term = taps_ref[k : k + 1, lanes] * padded[8 * j : 8 * j + own_q + 8, lanes]
                        part = term if part is None else part + term
                shifted[...] = part
                total = total + shifted[r : r + own_q, :]
            conv[:, lanes] = total
        whole = conv[...]
        mean = jnp.sum(whole, axis=1, keepdims=True) / channels
        off = whole - mean
        spread = jnp.sum(off * off, axis=1, keepdims=True)
        lane = lax.broadcasted_iota(jnp.int32, (own_q, 128), 1)
        moments[tp] = jnp.transpose(jnp.where(lane == 0, mean, spread))[:8]

    def moment_copy(i):
        at = moments.at[tp]
        return remote(at, at, sent_m.at[i], got_m.at[tp], others[i])

    def activate():
        for i in range(1, 4):
            source = lax.rem(tp + i, 4)
            at = moments.at[source]
            remote(at, at, sent_m.at[0], got_m.at[source], others[0]).wait_recv()
        means = [moments[n, 0:1, :] for n in range(4)]
        mean = sum(means) / 4
        apart = sum((m - mean) * (m - mean) for m in means)
        spread = (sum(moments[n, 1:2, :] for n in range(4)) + channels * apart) / (4 * channels)
        tall = lambda row: jnp.transpose(jnp.broadcast_to(row, (128, own_q)))
        mean, scaling = tall(mean), tall(lax.rsqrt(spread + eps_layer))
        for at in range(0, channels, 128):
            lanes = slice(at, at + 128)
            value = (conv[:, lanes] - mean) * scaling * gain_ref[:, lanes]
            active[:, lanes] = jax.nn.silu(value).astype(bf16)
        for n in range(4):
            cols = slice(n * columns, (n + 1) * columns)
            cp_ref[:, cols] = jnp.dot(
                active[...], oc_ref[:, cols], preferred_element_type=f32
            ).astype(bf16)

    convolve()
    x_first(1)
    x_first(2)
    for i in range(3):
        moment_copy(i).start()
    expand(0)
    q_from(1, (1, 0))
    q_from(3, (0, 1))
    activate()
    x_first(3)
    x_first(4)
    for i in range(3):
        block_copy(1, i, cp_ref, conv_in).start()
    pair_arrived(0)

    blocks = (0, 1, 3, 1, 3, 1, 1, 2, 2, 2, 2, 3, 3, 0, 0, 0)
    chunks = (0, 0, 0, 1, 1, 2, 3, 0, 1, 2, 3, 2, 3, 1, 2, 3)

    def looked_up(step, values):
        found = values[0]
        for n in range(1, 16):
            if values[n] != values[n - 1]:
                found = found + (values[n] - values[n - 1]) * ((step + 16 - n) // 16)
        return found

    hooks = {
        1: lambda: pair_arrived(1),
        2: lambda: pair_arrived(3),
        3: lambda: (x_first(5), x_first(6), q_from(2, (0, 1)), expand(1)),
        5: lambda: (x_first(7), expand(2)),
        6: lambda: expand(3),
        7: lambda: (pair_arrived(2), swap_start(1)),
        8: lambda: merge(1),
        11: lambda: swap_start(2),
        12: lambda: merge(2),
        13: lambda: swap_start(3),
        14: lambda: merge(3),
    }

    @pl.loop(0, 16)
    def _(step):
        for n, hook in hooks.items():
            def run(hook=hook):
                hook()
            pl.when(step == n)(run)
        compute(looked_up(step, blocks), looked_up(step, chunks))

    swap_start(0)
    for copy in first:
        copy.wait_send()
    for i in range(3):
        moment_copy(i).wait_send()
        block_copy(1, i, cp_ref, conv_in).wait_send()
    for k in range(1, 8):
        for n in range(2):
            if goes(k, n):
                x_copy(k, n, up if k % 2 else down).wait_send()
    for n in range(2):
        relay_q(n).wait_send()
        for r in range(1, 4):
            pair_q(r, n).wait_send()
    for r in range(1, 4):
        for copy in part_copy(r):
            copy.wait()
    for copy in swap(0):
        copy.wait()
    for h in range(heads):
        tops = [high[0, h : h + 1, :own_q], high_in[0, h : h + 1, :]]
        totals = [acc[0, h, vrows : vrows + 1, :own_q], acc_in[0, h, vrows : vrows + 1, :]]
        for r in range(3):
            tops.append(stat_in[r, h, 4:5, :])
            totals.append(stat_in[r, h, 0:1, :])
        top = functools.reduce(jnp.maximum, tops)
        shares = [jnp.exp2((m - top) * scale) for m in tops]
        total = sum(t * a for t, a in zip(totals, shares))
        whole = acc[0, h, :vrows, :own_q] * shares[0] + acc_in[0, h, :vrows, :] * shares[1]
        for r in range(3):
            whole = whole + part_in[r, h].astype(f32) * (shares[2 + r] * totals[2 + r])
        wide[tp, :, h * vrows : (h + 1) * vrows] = jnp.transpose(whole / total).astype(bf16)
    last = [
        remote(wide.at[tp], wide.at[tp], sent_t.at[2, i], got_t.at[2, tp], peer)
        for i, peer in enumerate(others)
    ]
    for copy in last:
        copy.start()
    result = jnp.dot(wide[tp], block(wa_ref, tp)[...], preferred_element_type=f32)
    result = result + block(cp_ref, tp)[...].astype(f32)
    for i in (1, 3, 2):
        source = lax.rem(tp + i, 4)
        for kind, dst in enumerate((weight_in, conv_in, wide)):
            at = dst.at[source]
            remote(at, at, sent_t.at[kind, 0], got_t.at[kind, source], others[0]).wait_recv()
        result = result + jnp.dot(wide[source], weight_in[source], preferred_element_type=f32)
        result = result + conv_in[source].astype(f32)
    out_ref[...] = result.astype(bf16)
    for copy in last:
        copy.wait_send()


def attend(xp, qt, key_up, value_up_t, out_attend, glu, taps, bias, gain, out_conv, size):
    heads, width, own_q = qt.shape
    vdim = value_up_t.shape[0] // heads
    columns = out_attend.shape[1] // 4
    channels = glu.shape[1]
    vmem = pl.BlockSpec(memory_space=pltpu.VMEM)
    dma = pltpu.SemaphoreType.DMA
    scale = math.log2(math.e) * size ** (-0.5)
    return pl.pallas_call(
        functools.partial(attend_kernel, heads, scale),
        out_shape=jax.ShapeDtypeStruct((own_q, columns), bf16),
        in_specs=[vmem] * 10,
        out_specs=vmem,
        scratch_shapes=[
            pltpu.VMEM((8, *xp.shape), bf16),
            pltpu.VMEM((4, 2, heads, width, own_q), bf16),
            pltpu.VMEM((4, heads, 2 * own_q, width), bf16),
            pltpu.VMEM((4, heads, vdim + 16, 2 * own_q), bf16),
            pltpu.VMEM((4, heads, vdim + 16, 2 * own_q), f32),
            pltpu.VMEM((4, heads, 2 * own_q), f32),
            pltpu.VMEM((4, heads, vdim + 16, own_q), f32),
            pltpu.VMEM((4, heads, own_q), f32),
            pltpu.VMEM((3, heads, vdim, own_q), bf16),
            pltpu.VMEM((3, heads, 8, own_q), f32),
            pltpu.VMEM((3, heads, vdim, own_q), bf16),
            pltpu.VMEM((3, heads, 8, own_q), f32),
            pltpu.VMEM((4, own_q, heads * vdim), bf16),
            pltpu.VMEM((4, own_q, columns), bf16),
            pltpu.VMEM((4, heads * vdim, columns), bf16),
            pltpu.VMEM((2, 16, channels), bf16),
            pltpu.VMEM((own_q + 32, channels), f32),
            pltpu.VMEM((own_q + 8, 128), f32),
            pltpu.VMEM((own_q, channels), f32),
            pltpu.VMEM((4, 8, own_q), f32),
            pltpu.VMEM((own_q, channels), bf16),
            pltpu.VMEM((own_q, 4 * columns), bf16),
            dma((8, 2)),
            dma((8, 2)),
            dma((4, 2)),
            dma((2, 2)),
            dma((2,)),
            dma((4, 2)),
            dma((4, 2)),
            dma((4, 4)),
            dma((3, 2, 2)),
            dma((3, 3)),
            dma((3, 4)),
            dma((2, 2)),
            dma((3,)),
            dma((4,)),
        ],
        compiler_params=pltpu.CompilerParams(
            collective_id=0, has_side_effects=True, vmem_limit_bytes=56 * 2**20
        ),
        cost_estimate=pl.CostEstimate(
            flops=2 * 8192 * 2 * own_q * heads * 320,
            bytes_accessed=2 * 10**6,
            transcendentals=8192 * 2 * own_q * heads,
        ),
        name="attend",
    )(xp, qt, key_up, value_up_t, out_attend, glu, taps, bias[None], gain[None], out_conv)


def per_device(
    tokens,
    in_gain,
    query_down,
    latent_down,
    rope_down,
    query_gain,
    latent_gain,
    query_nope,
    query_rope,
    key_up,
    value_up,
    conv_value,
    conv_gate,
    conv_taps,
    conv_bias,
    channel_gain,
    out_attend,
    out_conv,
):
    row_count = tokens.shape[0]
    width = in_gain.shape[0]
    positions = (lax.axis_index("sp") * row_count + jnp.arange(row_count)).astype(f32)
    piece_f = gather_directly(tokens, "tp", 1).astype(f32)
    scaled = (piece_f * in_gain).astype(bf16)

    def add_rows(weight):
        return jnp.dot(scaled, weight, preferred_element_type=f32)

    square_sum = jnp.sum(piece_f * piece_f, axis=1)
    q_pre = add_rows(query_down)
    kv_pre = add_rows(latent_down)
    rope_pre = add_rows(rope_down)
    value_pre = add_rows(conv_value)
    gate_pre = add_rows(conv_gate)
    row_scale = lax.rsqrt(square_sum / width + eps_norm)[:, None]
    q_latent = rms_scale(row_scale * q_pre, query_gain).astype(bf16)
    kv_latent = rms_scale(row_scale * kv_pre, latent_gain).astype(bf16)
    rope_key = rotate(row_scale * rope_pre, positions).astype(bf16)
    rope_size = rope_down.shape[1]
    heads = query_rope.shape[1] // rope_size
    nope = query_nope.shape[1] // heads

    packed = jnp.transpose(rope_key.reshape(2, 8, 16, rope_size), (0, 2, 1, 3)).reshape(2, 16, 8 * rope_size)
    xp = jnp.concatenate([kv_latent.reshape(2, row_count // 2, -1), packed], axis=1)

    q_heads = (
        jnp.dot(q_latent, query_nope, preferred_element_type=f32)
        .astype(bf16)
        .reshape(row_count, heads, nope)
    )
    q_turn = jnp.dot(q_latent, query_rope, preferred_element_type=f32).reshape(
        row_count, heads, rope_size
    )
    r_heads = rotate(q_turn, positions[:, None]).astype(bf16)
    empty = jnp.zeros((row_count, 64 - rope_size), bf16)
    cols = []
    for h in range(heads):
        if h % 2 == 0:
            cols += [q_heads[:, h], r_heads[:, h], empty]
        else:
            cols += [r_heads[:, h], empty, q_heads[:, h]]
    q_own = jnp.transpose(jnp.concatenate(cols, axis=1))
    glu = (row_scale * value_pre * jax.nn.sigmoid(row_scale * gate_pre)).astype(bf16)
    return attend(
        xp,
        q_own.reshape(heads, 128, row_count),
        key_up,
        jnp.transpose(value_up),
        out_attend,
        glu,
        conv_taps,
        conv_bias,
        channel_gain,
        out_conv,
        nope + rope_size,
    )


def solution(mesh):
    in_specs = (
        P("sp", "tp"),
        P(),
        P(),
        P(),
        P(),
        P(),
        P(),
        P(None, "tp"),
        P(None, "tp"),
        P(None, "tp"),
        P(None, "tp"),
        P(None, "tp"),
        P(None, "tp"),
        P(None, "tp"),
        P("tp"),
        P("tp"),
        P("tp", None),
        P("tp", None),
    )
    return jax.shard_map(
        per_device, mesh=mesh, in_specs=in_specs, out_specs=P("sp", "tp"), check_vma=False
    )
```

```python
import functools
import math

import jax
import jax.numpy as jnp
from jax import lax
from jax.experimental import pallas as pl
from jax.experimental.pallas import tpu as pltpu
from jax.sharding import PartitionSpec as P

eps_norm = 1e-06
eps_layer = 1e-05
theta = 10000.0
bf16 = jnp.bfloat16
f32 = jnp.float32

def rms_scale(values, gain):
    return values * lax.rsqrt(jnp.mean(values * values, axis=-1, keepdims=True) + eps_norm) * gain


def rotate(values, positions):
    half = values.shape[-1] // 2
    freqs = theta ** (-jnp.arange(half).astype(f32) / half)
    angles = positions[..., None] * freqs
    cosine = jnp.cos(angles)
    sine = jnp.sin(angles)
    first = values[..., :half]
    second = values[..., half:]
    return jnp.concatenate(
        [first * cosine - second * sine, second * cosine + first * sine], axis=-1
    )


def attend_kernel(
    heads, scale, xp_ref, qt_ref, ku_ref, vut_ref, wa_ref, glu_ref,
    taps_ref, bias_ref, gain_ref, oc_ref, out_ref,
    x, q, keys, vals, acc, high, acc_in, high_in, part_out, stat_out, part_in, stat_in, wide, conv_in, weight_in,
    halo, padded, shifted, conv, moments, active, cp_ref,
    got_x, sent_x, got_q, sent_q, sent_relay, sent_pair_q, got_pair_q, pair_sem, part_sem,
    sent_t, got_t, halo_sem, sent_m, got_m,
):
    sp, tp = lax.axis_index("sp"), lax.axis_index("tp")
    core = lax.rem(sp, 2)
    y = lax.rem(sp // 2, 4)
    z = sp // 8
    own_q = qt_ref.shape[2]
    depth = xp_ref.shape[1] - 16
    vrows = vut_ref.shape[0] // heads
    half_heads = heads // 2

    def device(pz, py):
        return (((pz * 4 + py) * 2 + core), tp)

    def turn(a, n):
        return lax.rem(a + 2 * n, n)

    up, down = device(turn(z + 1, 8), y), device(turn(z - 1, 8), y)
    right, left = device(z, turn(y + 1, 4)), device(z, turn(y - 1, 4))
    across = device(z, turn(y + 2, 4))
    sibling = (sp + 1 - 2 * core, tp)

    def remote(src, dst, sent, got, target):
        return pltpu.make_async_remote_copy(
            src_ref=src, dst_ref=dst, send_sem=sent, recv_sem=got,
            device_id=target, device_id_type=pl.DeviceIdType.MESH,
        )

    barrier = pltpu.get_barrier_semaphore()
    others = [(sp, lax.rem(tp + i, 4)) for i in (1, 3, 2)]
    count = 64
    beside = [(lax.rem(sp + 1, count), tp), (lax.rem(sp + count - 1, count), tp)]
    peers = (up, down, right, left, across, sibling, *others, *beside)
    for peer in peers:
        pl.semaphore_signal(barrier, inc=1, device_id=peer, device_id_type=pl.DeviceIdType.MESH)
    pl.semaphore_wait(barrier, len(peers))

    def plane(k):
        return turn(z + (1 - 2 * lax.rem(k, 2)) * ((k + 1) // 2), 8)

    def x_copy(k, n, target):
        at = x.at[plane(k), n]
        return remote(at, at, sent_x.at[k, n], got_x.at[plane(k), n], target)

    def part_of(ref, n):
        return ref.at[n * half_heads : (n + 1) * half_heads]

    def q_slot(py, who, n):
        return q.at[py, who, n * half_heads : (n + 1) * half_heads]

    first = []
    for n in range(2):
        for way, target in enumerate((up, down)):
            first.append(
                remote(xp_ref.at[n], x.at[z, n], sent_x.at[7 * way, n], got_x.at[z, n], target)
            )
    for n in range(2):
        for way, target in enumerate((right, left)):
            m = n if way == 0 else 1 - n
            first.append(
                remote(part_of(qt_ref, m), q_slot(y, core, m), sent_q.at[way, m], got_q.at[y, m], target)
            )
    for n in range(2):
        first.append(
            remote(
                part_of(qt_ref, n), q_slot(y, core, n), sent_pair_q.at[0, n],
                got_pair_q.at[y, n], sibling,
            )
        )
    columns = out_ref.shape[1]

    def block(ref, n):
        return ref.at[:, pl.ds(pl.multiple_of(n * columns, columns), columns)]

    def block_copy(kind, i, src, dst):
        peer = others[i]
        return remote(block(src, peer[1]), dst.at[tp], sent_t.at[kind, i], got_t.at[kind, tp], peer)

    halos = [
        remote(
            glu_ref.at[own_q - 16 :] if n == 0 else glu_ref.at[:16],
            halo.at[n], halo_sem.at[n, 0], halo_sem.at[n, 1], beside[n],
        )
        for n in range(2)
    ]
    first = halos + first + [block_copy(0, i, wa_ref, weight_in) for i in range(3)]
    for copy in first:
        copy.start()
    x[z] = xp_ref[...]
    q[y, core] = qt_ref[...]
    acc[...] = jnp.zeros_like(acc)
    high[...] = jnp.full_like(high, -jnp.inf)

    def goes(k, n):
        return k < 5 or (k == 5 and n == 0) or (k == 6 and n == 1)

    def x_first(k):
        for n in range(2):
            copy = x_copy(k, n, up if k % 2 else down)
            copy.wait_recv()
            if goes(k, n):
                copy.start()

    def pair_q(r, n):
        py = turn(y + r, 4)
        at = q_slot(py, core, n)
        return remote(at, at, sent_pair_q.at[r, n], got_pair_q.at[py, n], sibling)

    def arrived_q(r, n):
        py = turn(y + r, 4)
        at = q_slot(py, core, n)
        remote(at, at, sent_relay.at[n], got_q.at[py, n], sibling).wait_recv()

    def relay_q(n):
        py = turn(y - 1 + 2 * n, 4)
        at = q_slot(py, core, n)
        return remote(at, at, sent_relay.at[n], got_q.at[py, n], right if n == 0 else left)

    def pair_arrived(r):
        py = turn(y + r, 4)
        for n in range(2):
            at = q_slot(py, 1 - core, n)
            remote(at, at, sent_relay.at[n], got_pair_q.at[py, n], sibling).wait_recv()

    def q_from(r, order):
        for n in order:
            arrived_q(r, n)
            if (r, n) in ((3, 0), (1, 1)):
                relay_q(n).start()
            pair_q(r, n).start()

    def swap(r):
        return [
            remote(
                acc.at[r, :, :, own_q:], acc_in.at[r], pair_sem.at[r, 0], pair_sem.at[r, 1], sibling
            ),
            remote(high.at[r, :, own_q:], high_in.at[r], pair_sem.at[r, 2], pair_sem.at[r, 3], sibling),
        ]

    def swap_start(r):
        for copy in swap(r):
            copy.start()

    def part_copy(r):
        return [
            remote(
                out.at[r - 1], into.at[r - 1], part_sem.at[r - 1, n, 0], part_sem.at[r - 1, n, 1],
                {1: right, 2: across, 3: left}[r],
            )
            for n, (out, into) in enumerate(((stat_out, stat_in), (part_out, part_in)))
        ]

    def merge(r):
        for copy in swap(r):
            copy.wait()
        for h in range(heads):
            m0, m1 = high[r, h : h + 1, :own_q], high_in[r, h : h + 1, :]
            top = jnp.maximum(m0, m1)
            a0, a1 = jnp.exp2((m0 - top) * scale), jnp.exp2((m1 - top) * scale)
            total = acc[r, h, vrows : vrows + 1, :own_q] * a0 + acc_in[r, h, vrows : vrows + 1, :] * a1
            whole = acc[r, h, :vrows, :own_q] * a0 + acc_in[r, h, :vrows, :] * a1
            part_out[r - 1, h] = (whole / total).astype(bf16)
            stat_out[r - 1, h] = jnp.concatenate([total] * 4 + [top] * 4, axis=0)
        for copy in part_copy(r):
            copy.start()

    def expand(c):
        at = [plane(2 * c), plane(2 * c + 1)]
        latent = jnp.concatenate([x[s, n, :depth, :] for s in at for n in range(2)], axis=0)
        k = jnp.dot(latent, ku_ref[...], preferred_element_type=f32).astype(bf16)
        vt = lax.dot_general(
            vut_ref[...], latent, (((1,), (1,)), ((), ())), preferred_element_type=f32
        ).astype(bf16)
        even, odd = [], []
        for s in at:
            for n in range(2):
                for half in range(2):
                    part = x[s, n, depth:, 128 * half : 128 * half + 128].astype(f32)
                    r1, r2, r3 = (pltpu.roll(part, 32 * m, 1) for m in (1, 2, 3))
                    even += [r2, r1, part, r3]
                    odd += [part, r3, r2, r1]
        even = jnp.concatenate(even, axis=0).astype(bf16)
        odd = jnp.concatenate(odd, axis=0).astype(bf16)
        lane = lax.broadcasted_iota(jnp.int32, even.shape, 1)
        for h in range(heads):
            pair = k[:, 128 * (h // 2) : 128 * (h // 2) + 128]
            keys[c, h] = (
                jnp.where(lane < 64, pair, even) if h % 2 == 0 else jnp.where(lane >= 64, pair, odd)
            )
            vals[c, h, :vrows, :] = vt[h * vrows : (h + 1) * vrows]
            vals[c, h, vrows:, :] = jnp.ones((16, vt.shape[1]), bf16)

    def compute(r, c):
        py = turn(y + r, 4)

        def score(h):
            both = jnp.concatenate([q[py, core, h], q[py, 1 - core, h]], axis=1)
            return jnp.dot(keys[c, h], both, preferred_element_type=f32)

        following = score(0)
        for h in range(heads):
            s = following
            if h + 1 < heads:
                following = score(h + 1)
            old = high[r, h : h + 1, :]
            new = jnp.maximum(old, jnp.max(s, axis=0, keepdims=True))
            alpha = jnp.exp2((old - new) * scale)
            p = jnp.exp2((s - new) * scale).astype(bf16)
            high[r, h : h + 1, :] = new
            acc[r, h] = acc[r, h] * alpha + jnp.dot(vals[c, h], p, preferred_element_type=f32)

    channels = glu_ref.shape[1]

    def convolve():
        for copy in halos:
            copy.wait_recv()
        padded[16 : 16 + own_q, :] = glu_ref[...].astype(f32)
        padded[:16, :] = jnp.where(sp > 0, halo[0].astype(f32), 0.0)
        padded[16 + own_q :, :] = jnp.where(sp < count - 1, halo[1].astype(f32), 0.0)
        taps = taps_ref.shape[0]
        for at in range(0, channels, 128):
            lanes = slice(at, at + 128)
            total = jnp.broadcast_to(bias_ref[:, lanes], (own_q, 128))
            for r in range(8):
                part = None
                for j in range(4):
                    k = 8 * j + r - 1
                    if 0 <= k < taps:
                        term = taps_ref[k : k + 1, lanes] * padded[8 * j : 8 * j + own_q + 8, lanes]
                        part = term if part is None else part + term
                shifted[...] = part
                total = total + shifted[r : r + own_q, :]
            conv[:, lanes] = total
        whole = conv[...]
        mean = jnp.sum(whole, axis=1, keepdims=True) / channels
        off = whole - mean
        spread = jnp.sum(off * off, axis=1, keepdims=True)
        lane = lax.broadcasted_iota(jnp.int32, (own_q, 128), 1)
        moments[tp] = jnp.transpose(jnp.where(lane == 0, mean, spread))[:8]

    def moment_copy(i):
        at = moments.at[tp]
        return remote(at, at, sent_m.at[i], got_m.at[tp], others[i])

    def activate():
        for i in range(1, 4):
            source = lax.rem(tp + i, 4)
            at = moments.at[source]
            remote(at, at, sent_m.at[0], got_m.at[source], others[0]).wait_recv()
        means = [moments[n, 0:1, :] for n in range(4)]
        mean = sum(means) / 4
        apart = sum((m - mean) * (m - mean) for m in means)
        spread = (sum(moments[n, 1:2, :] for n in range(4)) + channels * apart) / (4 * channels)
        tall = lambda row: jnp.transpose(jnp.broadcast_to(row, (128, own_q)))
        mean, scaling = tall(mean), tall(lax.rsqrt(spread + eps_layer))
        for at in range(0, channels, 128):
            lanes = slice(at, at + 128)
            value = (conv[:, lanes] - mean) * scaling * gain_ref[:, lanes]
            active[:, lanes] = jax.nn.silu(value).astype(bf16)
        for n in range(4):
            cols = slice(n * columns, (n + 1) * columns)
            cp_ref[:, cols] = jnp.dot(
                active[...], oc_ref[:, cols], preferred_element_type=f32
            ).astype(bf16)

    convolve()
    x_first(1)
    x_first(2)
    for i in range(3):
        moment_copy(i).start()
    expand(0)
    q_from(1, (1, 0))
    q_from(3, (0, 1))
    activate()
    x_first(3)
    x_first(4)
    for i in range(3):
        block_copy(1, i, cp_ref, conv_in).start()
    pair_arrived(0)

    blocks = (0, 1, 3, 1, 3, 1, 1, 2, 2, 2, 2, 3, 3, 0, 0, 0)
    chunks = (0, 0, 0, 1, 1, 2, 3, 0, 1, 2, 3, 2, 3, 1, 2, 3)

    def looked_up(step, values):
        found = values[0]
        for n in range(1, 16):
            if values[n] != values[n - 1]:
                found = found + (values[n] - values[n - 1]) * ((step + 16 - n) // 16)
        return found

    hooks = {
        1: lambda: pair_arrived(1),
        2: lambda: pair_arrived(3),
        3: lambda: (x_first(5), x_first(6), q_from(2, (0, 1)), expand(1)),
        5: lambda: (x_first(7), expand(2)),
        6: lambda: expand(3),
        7: lambda: (pair_arrived(2), swap_start(1)),
        8: lambda: merge(1),
        11: lambda: swap_start(2),
        12: lambda: merge(2),
        13: lambda: swap_start(3),
        14: lambda: merge(3),
    }

    @pl.loop(0, 16)
    def _(step):
        for n, hook in hooks.items():
            def run(hook=hook):
                hook()
            pl.when(step == n)(run)
        compute(looked_up(step, blocks), looked_up(step, chunks))

    swap_start(0)
    for copy in first:
        copy.wait_send()
    for i in range(3):
        moment_copy(i).wait_send()
        block_copy(1, i, cp_ref, conv_in).wait_send()
    for k in range(1, 8):
        for n in range(2):
            if goes(k, n):
                x_copy(k, n, up if k % 2 else down).wait_send()
    for n in range(2):
        relay_q(n).wait_send()
        for r in range(1, 4):
            pair_q(r, n).wait_send()
    for r in range(1, 4):
        for copy in part_copy(r):
            copy.wait()
    for copy in swap(0):
        copy.wait()
    for h in range(heads):
        tops = [high[0, h : h + 1, :own_q], high_in[0, h : h + 1, :]]
        totals = [acc[0, h, vrows : vrows + 1, :own_q], acc_in[0, h, vrows : vrows + 1, :]]
        for r in range(3):
            tops.append(stat_in[r, h, 4:5, :])
            totals.append(stat_in[r, h, 0:1, :])
        top = functools.reduce(jnp.maximum, tops)
        shares = [jnp.exp2((m - top) * scale) for m in tops]
        total = sum(t * a for t, a in zip(totals, shares))
        whole = acc[0, h, :vrows, :own_q] * shares[0] + acc_in[0, h, :vrows, :] * shares[1]
        for r in range(3):
            whole = whole + part_in[r, h].astype(f32) * (shares[2 + r] * totals[2 + r])
        wide[tp, :, h * vrows : (h + 1) * vrows] = jnp.transpose(whole / total).astype(bf16)
    last = [
        remote(wide.at[tp], wide.at[tp], sent_t.at[2, i], got_t.at[2, tp], peer)
        for i, peer in enumerate(others)
    ]
    for copy in last:
        copy.start()
    result = jnp.dot(wide[tp], block(wa_ref, tp)[...], preferred_element_type=f32)
    result = result + block(cp_ref, tp)[...].astype(f32)
    for i in (1, 3, 2):
        source = lax.rem(tp + i, 4)
        for kind, dst in enumerate((weight_in, conv_in, wide)):
            at = dst.at[source]
            remote(at, at, sent_t.at[kind, 0], got_t.at[kind, source], others[0]).wait_recv()
        result = result + jnp.dot(wide[source], weight_in[source], preferred_element_type=f32)
        result = result + conv_in[source].astype(f32)
    out_ref[...] = result.astype(bf16)
    for copy in last:
        copy.wait_send()


def attend(xp, qt, key_up, value_up_t, out_attend, glu, taps, bias, gain, out_conv, size):
    heads, width, own_q = qt.shape
    vdim = value_up_t.shape[0] // heads
    columns = out_attend.shape[1] // 4
    channels = glu.shape[1]
    vmem = pl.BlockSpec(memory_space=pltpu.VMEM)
    dma = pltpu.SemaphoreType.DMA
    scale = math.log2(math.e) * size ** (-0.5)
    return pl.pallas_call(
        functools.partial(attend_kernel, heads, scale),
        out_shape=jax.ShapeDtypeStruct((own_q, columns), bf16),
        in_specs=[vmem] * 10,
        out_specs=vmem,
        scratch_shapes=[
            pltpu.VMEM((8, *xp.shape), bf16),
            pltpu.VMEM((4, 2, heads, width, own_q), bf16),
            pltpu.VMEM((4, heads, 2 * own_q, width), bf16),
            pltpu.VMEM((4, heads, vdim + 16, 2 * own_q), bf16),
            pltpu.VMEM((4, heads, vdim + 16, 2 * own_q), f32),
            pltpu.VMEM((4, heads, 2 * own_q), f32),
            pltpu.VMEM((4, heads, vdim + 16, own_q), f32),
            pltpu.VMEM((4, heads, own_q), f32),
            pltpu.VMEM((3, heads, vdim, own_q), bf16),
            pltpu.VMEM((3, heads, 8, own_q), f32),
            pltpu.VMEM((3, heads, vdim, own_q), bf16),
            pltpu.VMEM((3, heads, 8, own_q), f32),
            pltpu.VMEM((4, own_q, heads * vdim), bf16),
            pltpu.VMEM((4, own_q, columns), bf16),
            pltpu.VMEM((4, heads * vdim, columns), bf16),
            pltpu.VMEM((2, 16, channels), bf16),
            pltpu.VMEM((own_q + 32, channels), f32),
            pltpu.VMEM((own_q + 8, 128), f32),
            pltpu.VMEM((own_q, channels), f32),
            pltpu.VMEM((4, 8, own_q), f32),
            pltpu.VMEM((own_q, channels), bf16),
            pltpu.VMEM((own_q, 4 * columns), bf16),
            dma((8, 2)),
            dma((8, 2)),
            dma((4, 2)),
            dma((2, 2)),
            dma((2,)),
            dma((4, 2)),
            dma((4, 2)),
            dma((4, 4)),
            dma((3, 2, 2)),
            dma((3, 3)),
            dma((3, 4)),
            dma((2, 2)),
            dma((3,)),
            dma((4,)),
        ],
        compiler_params=pltpu.CompilerParams(
            collective_id=0, has_side_effects=True, vmem_limit_bytes=40 * 2**20
        ),
        cost_estimate=pl.CostEstimate(
            flops=2 * 8192 * 2 * own_q * heads * 320,
            bytes_accessed=2 * 10**6,
            transcendentals=8192 * 2 * own_q * heads,
        ),
        name="attend",
    )(xp, qt, key_up, value_up_t, out_attend, glu, taps, bias[None], gain[None], out_conv)


def project_kernel(
    tok_ref, gain_ref, qg_ref, lg_ref, wq_ref, wl_ref, wr_ref, wv_ref, wg_ref,
    q_ref, kv_ref, rope_ref, glu_ref,
    blocks, wq, wl, wr, wv, wg, aq, al, ar, av, ag, squares,
    sent, got, sent_relay, local,
):
    sp, tp = lax.axis_index("sp"), lax.axis_index("tp")
    width = tok_ref.shape[2]
    half = tok_ref.shape[1]

    def turn(a):
        return lax.rem(a + 4, 4)

    sides = [(sp, turn(tp + 1)), (sp, turn(tp - 1))]
    barrier = pltpu.get_barrier_semaphore()
    for peer in sides:
        pl.semaphore_signal(barrier, inc=1, device_id=peer, device_id_type=pl.DeviceIdType.MESH)
    pl.semaphore_wait(barrier, 2)

    def remote(src, at, n, sem, target):
        return pltpu.make_async_remote_copy(
            src_ref=src, dst_ref=blocks.at[at, n], send_sem=sem, recv_sem=got.at[at, n],
            device_id=target, device_id_type=pl.DeviceIdType.MESH,
        )

    first = [
        remote(tok_ref.at[m], tp, m, sent.at[way, m], sides[way])
        for n in range(2)
        for way, m in ((0, n), (1, 1 - n))
    ]
    for copy in first:
        copy.start()
    loads = [
        pltpu.make_async_copy(a, b, local.at[i])
        for i, (a, b) in enumerate(
            ((wq_ref, wq), (wl_ref, wl), (wr_ref, wr), (wv_ref, wv), (wg_ref, wg))
        )
    ]
    for copy in loads:
        copy.start()

    def relay(n):
        source = turn(tp - 1 + 2 * n)
        return remote(blocks.at[source, n], source, n, sent_relay.at[n], sides[n])

    def arrived(offset, n):
        source = turn(tp + offset)
        remote(blocks.at[source, n], source, n, sent_relay.at[n], sides[n]).wait_recv()

    def add(source, piece, n, fresh):
        here = slice(n * half, (n + 1) * half)
        value = piece.astype(f32)
        scaled = (value * gain_ref[source]).astype(bf16)
        square = jnp.broadcast_to(jnp.sum(value * value, axis=1, keepdims=True), (half, 128))
        rows = pl.ds(pl.multiple_of(source * width, width), width)
        squares[here] = square if fresh else squares[here] + square
        for w, a in ((wq, aq), (wl, al), (wr, ar), (wv, av), (wg, ag)):
            if w is wr:
                part = lax.dot_general(
                    scaled, w[:, rows], (((1,), (1,)), ((), ())), preferred_element_type=f32
                )
            else:
                part = jnp.dot(scaled, w[rows, :], preferred_element_type=f32)
            a[here] = part if fresh else a[here] + part

    for copy in loads:
        copy.wait()
    for n in range(2):
        add(tp, tok_ref[n], n, True)
    arrived(-1, 0)
    relay(0).start()
    arrived(1, 1)
    relay(1).start()
    left, right, across = turn(tp - 1), turn(tp + 1), turn(tp + 2)
    add(left, blocks[left, 0], 0, False)
    add(right, blocks[right, 1], 1, False)
    arrived(-1, 1)
    add(left, blocks[left, 1], 1, False)
    arrived(1, 0)
    add(right, blocks[right, 0], 0, False)
    for n in range(2):
        arrived(2, n)
        add(across, blocks[across, n], n, False)
    row_scale = lax.rsqrt(squares[:, :1] / (4 * width) + eps_norm)
    q_ref[...] = rms_scale(row_scale * aq[...], qg_ref[...]).astype(bf16)
    kv_ref[...] = rms_scale(row_scale * al[...], lg_ref[...]).astype(bf16)
    rope_ref[...] = row_scale * ar[...]
    glu_ref[...] = (row_scale * av[...] * jax.nn.sigmoid(row_scale * ag[...])).astype(bf16)
    for copy in first:
        copy.wait_send()
    for n in range(2):
        relay(n).wait_send()


def project(tokens, in_gain, query_gain, latent_gain, weights):
    rows, width = tokens.shape
    vmem = pl.BlockSpec(memory_space=pltpu.VMEM)
    dma = pltpu.SemaphoreType.DMA
    wide = [min(w.shape) for w in weights]
    return pl.pallas_call(
        project_kernel,
        out_shape=(
            jax.ShapeDtypeStruct((rows, wide[0]), bf16),
            jax.ShapeDtypeStruct((rows, wide[1]), bf16),
            jax.ShapeDtypeStruct((rows, wide[2]), f32),
            jax.ShapeDtypeStruct((rows, wide[3]), bf16),
        ),
        in_specs=[vmem] * 4 + [pl.BlockSpec(memory_space=pl.ANY)] * 5,
        out_specs=(vmem,) * 4,
        scratch_shapes=[pltpu.VMEM((4, 2, rows // 2, width), bf16)]
        + [pltpu.VMEM(w.shape, bf16) for w in weights]
        + [pltpu.VMEM((rows, n), f32) for n in wide]
        + [pltpu.VMEM((rows, 128), f32), dma((2, 2)), dma((4, 2)), dma((2,)), dma((5,))],
        compiler_params=pltpu.CompilerParams(
            collective_id=1, has_side_effects=True, vmem_limit_bytes=60 * 2**20
        ),
        cost_estimate=pl.CostEstimate(
            flops=2 * rows * 4 * width * sum(wide), bytes_accessed=10**7, transcendentals=10**5
        ),
        name="project",
    )(
        tokens.reshape(2, rows // 2, width),
        in_gain.reshape(4, 1, width),
        query_gain[None],
        latent_gain[None],
        *weights,
    )


def per_device(
    tokens,
    in_gain,
    query_down,
    latent_down,
    rope_down,
    query_gain,
    latent_gain,
    query_nope,
    query_rope,
    key_up,
    value_up,
    conv_value,
    conv_gate,
    conv_taps,
    conv_bias,
    channel_gain,
    out_attend,
    out_conv,
):
    row_count = tokens.shape[0]
    positions = (lax.axis_index("sp") * row_count + jnp.arange(row_count)).astype(f32)
    q_latent, kv_latent, rope_pre, glu = project(
        tokens,
        in_gain,
        query_gain,
        latent_gain,
        (query_down, latent_down, jnp.transpose(rope_down), conv_value, conv_gate),
    )
    rope_key = rotate(rope_pre, positions).astype(bf16)
    rope_size = rope_down.shape[1]
    heads = query_rope.shape[1] // rope_size
    nope = query_nope.shape[1] // heads

    packed = jnp.transpose(rope_key.reshape(2, 8, 16, rope_size), (0, 2, 1, 3)).reshape(2, 16, 8 * rope_size)
    xp = jnp.concatenate([kv_latent.reshape(2, row_count // 2, -1), packed], axis=1)

    q_heads = (
        jnp.dot(q_latent, query_nope, preferred_element_type=f32)
        .astype(bf16)
        .reshape(row_count, heads, nope)
    )
    q_turn = jnp.dot(q_latent, query_rope, preferred_element_type=f32).reshape(
        row_count, heads, rope_size
    )
    r_heads = rotate(q_turn, positions[:, None]).astype(bf16)
    empty = jnp.zeros((row_count, 64 - rope_size), bf16)
    cols = []
    for h in range(heads):
        if h % 2 == 0:
            cols += [q_heads[:, h], r_heads[:, h], empty]
        else:
            cols += [r_heads[:, h], empty, q_heads[:, h]]
    q_own = jnp.transpose(jnp.concatenate(cols, axis=1))
    return attend(
        xp,
        q_own.reshape(heads, 128, row_count),
        key_up,
        jnp.transpose(value_up),
        out_attend,
        glu,
        conv_taps,
        conv_bias,
        channel_gain,
        out_conv,
        nope + rope_size,
    )


def solution(mesh):
    in_specs = (
        P("sp", "tp"),
        P(),
        P(),
        P(),
        P(),
        P(),
        P(),
        P(None, "tp"),
        P(None, "tp"),
        P(None, "tp"),
        P(None, "tp"),
        P(None, "tp"),
        P(None, "tp"),
        P(None, "tp"),
        P("tp"),
        P("tp"),
        P("tp", None),
        P("tp", None),
    )
    return jax.shard_map(
        per_device, mesh=mesh, in_specs=in_specs, out_specs=P("sp", "tp"), check_vma=False
    )
```

```python
import functools
import math

import jax
import jax.numpy as jnp
from jax import lax
from jax.experimental import pallas as pl
from jax.experimental.pallas import tpu as pltpu
from jax.sharding import PartitionSpec as P

eps_norm = 1e-06
eps_layer = 1e-05
theta = 10000.0
bf16 = jnp.bfloat16
f32 = jnp.float32

def rms_scale(values, gain):
    return values * lax.rsqrt(jnp.mean(values * values, axis=-1, keepdims=True) + eps_norm) * gain


def rotate(values, positions):
    half = values.shape[-1] // 2
    freqs = theta ** (-jnp.arange(half).astype(f32) / half)
    angles = positions[..., None] * freqs
    cosine = jnp.cos(angles)
    sine = jnp.sin(angles)
    first = values[..., :half]
    second = values[..., half:]
    return jnp.concatenate(
        [first * cosine - second * sine, second * cosine + first * sine], axis=-1
    )


def attend_kernel(
    heads, scale, xp_ref, qt_ref, ku_ref, vu_ref, wa_ref, glu_ref,
    taps_ref, bias_ref, gain_ref, oc_ref, out_ref,
    x, q, keys, vals, acc, high, acc_in, high_in, part_out, stat_out, part_in, stat_in, wide, conv_in, weight_in,
    halo, padded, shifted, conv, moments, active, cp_ref, vut_ref,
    got_x, sent_x, got_q, sent_q, sent_relay, sent_pair_q, got_pair_q, pair_sem, part_sem,
    sent_t, got_t, halo_sem, sent_m, got_m, sent_f, got_f, relay_f,
):
    sp, tp = lax.axis_index("sp"), lax.axis_index("tp")
    core = lax.rem(sp, 2)
    y = lax.rem(sp // 2, 4)
    z = sp // 8
    own_q = qt_ref.shape[2]
    depth = xp_ref.shape[1] - 16
    vrows = vu_ref.shape[1] // heads
    half_heads = heads // 2

    def device(pz, py):
        return (((pz * 4 + py) * 2 + core), tp)

    def turn(a, n):
        return lax.rem(a + 2 * n, n)

    up, down = device(turn(z + 1, 8), y), device(turn(z - 1, 8), y)
    right, left = device(z, turn(y + 1, 4)), device(z, turn(y - 1, 4))
    across = device(z, turn(y + 2, 4))
    sibling = (sp + 1 - 2 * core, tp)

    def remote(src, dst, sent, got, target):
        return pltpu.make_async_remote_copy(
            src_ref=src, dst_ref=dst, send_sem=sent, recv_sem=got,
            device_id=target, device_id_type=pl.DeviceIdType.MESH,
        )

    barrier = pltpu.get_barrier_semaphore()
    others = [(sp, lax.rem(tp + i, 4)) for i in (1, 3, 2)]
    count = 64
    beside = [(lax.rem(sp + 1, count), tp), (lax.rem(sp + count - 1, count), tp)]
    peers = (up, down, right, left, across, sibling, *others, *beside)
    for peer in peers:
        pl.semaphore_signal(barrier, inc=1, device_id=peer, device_id_type=pl.DeviceIdType.MESH)
    pl.semaphore_wait(barrier, len(peers))

    def plane(k):
        return turn(z + (1 - 2 * lax.rem(k, 2)) * ((k + 1) // 2), 8)

    def x_copy(k, n, target):
        at = x.at[plane(k), n]
        return remote(at, at, sent_x.at[k, n], got_x.at[plane(k), n], target)

    def part_of(ref, n):
        return ref.at[n * half_heads : (n + 1) * half_heads]

    def q_slot(py, who, n):
        return q.at[py, who, n * half_heads : (n + 1) * half_heads]

    first = []
    for n in range(2):
        for way, target in enumerate((up, down)):
            first.append(
                remote(xp_ref.at[n], x.at[z, n], sent_x.at[7 * way, n], got_x.at[z, n], target)
            )
    for n in range(2):
        for way, target in enumerate((right, left)):
            m = n if way == 0 else 1 - n
            first.append(
                remote(part_of(qt_ref, m), q_slot(y, core, m), sent_q.at[way, m], got_q.at[y, m], target)
            )
    for n in range(2):
        first.append(
            remote(
                part_of(qt_ref, n), q_slot(y, core, n), sent_pair_q.at[0, n],
                got_pair_q.at[y, n], sibling,
            )
        )
    columns = out_ref.shape[1]

    def block(ref, n):
        return ref.at[:, pl.ds(pl.multiple_of(n * columns, columns), columns)]

    def block_copy(kind, i, src, dst):
        peer = others[i]
        return remote(block(src, peer[1]), dst.at[tp], sent_t.at[kind, i], got_t.at[kind, tp], peer)

    halos = [
        remote(
            glu_ref.at[own_q - 16 :] if n == 0 else glu_ref.at[:16],
            halo.at[n], halo_sem.at[n, 0], halo_sem.at[n, 1], beside[n],
        )
        for n in range(2)
    ]
    first = halos + first + [block_copy(0, i, wa_ref, weight_in) for i in range(3)]
    for copy in first:
        copy.start()
    x[z] = xp_ref[...]
    q[y, core] = qt_ref[...]
    vut_ref[...] = jnp.transpose(vu_ref[...].astype(f32)).astype(bf16)
    acc[...] = jnp.zeros_like(acc)
    high[...] = jnp.full_like(high, -jnp.inf)

    def goes(k, n):
        return k < 5 or (k == 5 and n == 0) or (k == 6 and n == 1)

    def x_first(k):
        for n in range(2):
            copy = x_copy(k, n, up if k % 2 else down)
            copy.wait_recv()
            if goes(k, n):
                copy.start()

    def pair_q(r, n):
        py = turn(y + r, 4)
        at = q_slot(py, core, n)
        return remote(at, at, sent_pair_q.at[r, n], got_pair_q.at[py, n], sibling)

    def arrived_q(r, n):
        py = turn(y + r, 4)
        at = q_slot(py, core, n)
        remote(at, at, sent_relay.at[n], got_q.at[py, n], sibling).wait_recv()

    def relay_q(n):
        py = turn(y - 1 + 2 * n, 4)
        at = q_slot(py, core, n)
        return remote(at, at, sent_relay.at[n], got_q.at[py, n], right if n == 0 else left)

    def pair_arrived(r):
        py = turn(y + r, 4)
        for n in range(2):
            at = q_slot(py, 1 - core, n)
            remote(at, at, sent_relay.at[n], got_pair_q.at[py, n], sibling).wait_recv()

    def q_from(r, order):
        for n in order:
            arrived_q(r, n)
            if (r, n) in ((3, 0), (1, 1)):
                relay_q(n).start()
            pair_q(r, n).start()

    def swap(r):
        return [
            remote(
                acc.at[r, :, :, own_q:], acc_in.at[r], pair_sem.at[r, 0], pair_sem.at[r, 1], sibling
            ),
            remote(high.at[r, :, own_q:], high_in.at[r], pair_sem.at[r, 2], pair_sem.at[r, 3], sibling),
        ]

    def swap_start(r):
        for copy in swap(r):
            copy.start()

    def part_copy(r):
        return [
            remote(
                out.at[r - 1], into.at[r - 1], part_sem.at[r - 1, n, 0], part_sem.at[r - 1, n, 1],
                {1: right, 2: across, 3: left}[r],
            )
            for n, (out, into) in enumerate(((stat_out, stat_in), (part_out, part_in)))
        ]

    def merge(r):
        for copy in swap(r):
            copy.wait()
        for h in range(heads):
            m0, m1 = high[r, h : h + 1, :own_q], high_in[r, h : h + 1, :]
            top = jnp.maximum(m0, m1)
            a0, a1 = jnp.exp2((m0 - top) * scale), jnp.exp2((m1 - top) * scale)
            total = acc[r, h, vrows : vrows + 1, :own_q] * a0 + acc_in[r, h, vrows : vrows + 1, :] * a1
            whole = acc[r, h, :vrows, :own_q] * a0 + acc_in[r, h, :vrows, :] * a1
            part_out[r - 1, h] = (whole / total).astype(bf16)
            stat_out[r - 1, h] = jnp.concatenate([total] * 4 + [top] * 4, axis=0)
        for copy in part_copy(r):
            copy.start()

    def expand(c):
        at = [plane(2 * c), plane(2 * c + 1)]
        latent = jnp.concatenate([x[s, n, :depth, :] for s in at for n in range(2)], axis=0)
        k = jnp.dot(latent, ku_ref[...], preferred_element_type=f32).astype(bf16)
        vt = lax.dot_general(
            vut_ref[...], latent, (((1,), (1,)), ((), ())), preferred_element_type=f32
        ).astype(bf16)
        even, odd = [], []
        for s in at:
            for n in range(2):
                for half in range(2):
                    part = x[s, n, depth:, 128 * half : 128 * half + 128].astype(f32)
                    r1, r2, r3 = (pltpu.roll(part, 32 * m, 1) for m in (1, 2, 3))
                    even += [r2, r1, part, r3]
                    odd += [part, r3, r2, r1]
        even = jnp.concatenate(even, axis=0).astype(bf16)
        odd = jnp.concatenate(odd, axis=0).astype(bf16)
        lane = lax.broadcasted_iota(jnp.int32, even.shape, 1)
        for h in range(heads):
            pair = k[:, 128 * (h // 2) : 128 * (h // 2) + 128]
            keys[c, h] = (
                jnp.where(lane < 64, pair, even) if h % 2 == 0 else jnp.where(lane >= 64, pair, odd)
            )
            vals[c, h, :vrows, :] = vt[h * vrows : (h + 1) * vrows]
            vals[c, h, vrows:, :] = jnp.ones((16, vt.shape[1]), bf16)

    def compute(r, c):
        py = turn(y + r, 4)

        def score(h):
            both = jnp.concatenate([q[py, core, h], q[py, 1 - core, h]], axis=1)
            return jnp.dot(keys[c, h], both, preferred_element_type=f32)

        following = score(0)
        for h in range(heads):
            s = following
            if h + 1 < heads:
                following = score(h + 1)
            old = high[r, h : h + 1, :]
            new = jnp.maximum(old, jnp.max(s, axis=0, keepdims=True))
            alpha = jnp.exp2((old - new) * scale)
            p = jnp.exp2((s - new) * scale).astype(bf16)
            high[r, h : h + 1, :] = new
            acc[r, h] = acc[r, h] * alpha + jnp.dot(vals[c, h], p, preferred_element_type=f32)

    channels = glu_ref.shape[1]

    def convolve():
        for copy in halos:
            copy.wait_recv()
        padded[16 : 16 + own_q, :] = glu_ref[...].astype(f32)
        padded[:16, :] = jnp.where(sp > 0, halo[0].astype(f32), 0.0)
        padded[16 + own_q :, :] = jnp.where(sp < count - 1, halo[1].astype(f32), 0.0)
        taps = taps_ref.shape[0]
        for at in range(0, channels, 128):
            lanes = slice(at, at + 128)
            total = jnp.broadcast_to(bias_ref[:, lanes], (own_q, 128))
            for r in range(8):
                part = None
                for j in range(4):
                    k = 8 * j + r - 1
                    if 0 <= k < taps:
                        term = taps_ref[k : k + 1, lanes] * padded[8 * j : 8 * j + own_q + 8, lanes]
                        part = term if part is None else part + term
                shifted[...] = part
                total = total + shifted[r : r + own_q, :]
            conv[:, lanes] = total
        whole = conv[...]
        mean = jnp.sum(whole, axis=1, keepdims=True) / channels
        off = whole - mean
        spread = jnp.sum(off * off, axis=1, keepdims=True)
        lane = lax.broadcasted_iota(jnp.int32, (own_q, 128), 1)
        moments[tp] = jnp.transpose(jnp.where(lane == 0, mean, spread))[:8]

    def moment_copy(i):
        at = moments.at[tp]
        return remote(at, at, sent_m.at[i], got_m.at[tp], others[i])

    def activate():
        for i in range(1, 4):
            source = lax.rem(tp + i, 4)
            at = moments.at[source]
            remote(at, at, sent_m.at[0], got_m.at[source], others[0]).wait_recv()
        means = [moments[n, 0:1, :] for n in range(4)]
        mean = sum(means) / 4
        apart = sum((m - mean) * (m - mean) for m in means)
        spread = (sum(moments[n, 1:2, :] for n in range(4)) + channels * apart) / (4 * channels)
        tall = lambda row: jnp.transpose(jnp.broadcast_to(row, (128, own_q)))
        mean, scaling = tall(mean), tall(lax.rsqrt(spread + eps_layer))
        for at in range(0, channels, 128):
            lanes = slice(at, at + 128)
            value = (conv[:, lanes] - mean) * scaling * gain_ref[:, lanes]
            active[:, lanes] = jax.nn.silu(value).astype(bf16)
        for n in range(4):
            cols = slice(n * columns, (n + 1) * columns)
            cp_ref[:, cols] = jnp.dot(
                active[...], oc_ref[:, cols], preferred_element_type=f32
            ).astype(bf16)

    convolve()
    x_first(1)
    x_first(2)
    for i in range(3):
        moment_copy(i).start()
    expand(0)
    q_from(1, (1, 0))
    q_from(3, (0, 1))
    activate()
    x_first(3)
    x_first(4)
    for i in range(3):
        block_copy(1, i, cp_ref, conv_in).start()
    pair_arrived(0)

    blocks = (0, 1, 3, 1, 3, 1, 1, 2, 2, 2, 2, 3, 3, 0, 0, 0)
    chunks = (0, 0, 0, 1, 1, 2, 3, 0, 1, 2, 3, 2, 3, 1, 2, 3)

    def looked_up(step, values):
        found = values[0]
        for n in range(1, 16):
            if values[n] != values[n - 1]:
                found = found + (values[n] - values[n - 1]) * ((step + 16 - n) // 16)
        return found

    hooks = {
        1: lambda: pair_arrived(1),
        2: lambda: pair_arrived(3),
        3: lambda: (x_first(5), x_first(6), q_from(2, (0, 1)), expand(1)),
        5: lambda: (x_first(7), expand(2)),
        6: lambda: expand(3),
        7: lambda: (pair_arrived(2), swap_start(1)),
        8: lambda: merge(1),
        11: lambda: swap_start(2),
        12: lambda: merge(2),
        13: lambda: swap_start(3),
        14: lambda: merge(3),
    }

    @pl.loop(0, 16)
    def _(step):
        for n, hook in hooks.items():
            def run(hook=hook):
                hook()
            pl.when(step == n)(run)
        compute(looked_up(step, blocks), looked_up(step, chunks))

    swap_start(0)
    for copy in first:
        copy.wait_send()
    for i in range(3):
        moment_copy(i).wait_send()
        block_copy(1, i, cp_ref, conv_in).wait_send()
    for k in range(1, 8):
        for n in range(2):
            if goes(k, n):
                x_copy(k, n, up if k % 2 else down).wait_send()
    for n in range(2):
        relay_q(n).wait_send()
        for r in range(1, 4):
            pair_q(r, n).wait_send()
    for r in range(1, 4):
        for copy in part_copy(r):
            copy.wait()
    for copy in swap(0):
        copy.wait()
    half = own_q // 2
    for h in range(heads):
        tops = [high[0, h : h + 1, :own_q], high_in[0, h : h + 1, :]]
        totals = [acc[0, h, vrows : vrows + 1, :own_q], acc_in[0, h, vrows : vrows + 1, :]]
        for r in range(3):
            tops.append(stat_in[r, h, 4:5, :])
            totals.append(stat_in[r, h, 0:1, :])
        top = functools.reduce(jnp.maximum, tops)
        shares = [jnp.exp2((m - top) * scale) for m in tops]
        total = sum(t * a for t, a in zip(totals, shares))
        whole = acc[0, h, :vrows, :own_q] * shares[0] + acc_in[0, h, :vrows, :] * shares[1]
        for r in range(3):
            whole = whole + part_in[r, h].astype(f32) * (shares[2 + r] * totals[2 + r])
        done = jnp.transpose(whole / total).astype(bf16)
        for n in range(2):
            wide[tp, n, :, h * vrows : (h + 1) * vrows] = done[n * half : (n + 1) * half]
    def final_copy(source, n, sem, target):
        at = wide.at[source, n]
        return remote(at, at, sem, got_f.at[source, n], target)

    sides = others[:2]
    last = [
        final_copy(tp, m, sent_f.at[way, m], sides[way])
        for n in range(2)
        for way, m in ((0, n), (1, 1 - n))
    ]
    for copy in last:
        copy.start()
    own_weight = block(wa_ref, tp)[...]
    around = [lax.rem(tp + i, 4) for i in (1, 2, 3)]
    for source in around:
        for kind, dst in enumerate((weight_in, conv_in)):
            at = dst.at[source]
            remote(at, at, sent_t.at[kind, 0], got_t.at[kind, source], others[0]).wait_recv()
    result = []
    for n in range(2):
        rows = slice(n * half, (n + 1) * half)
        part = jnp.dot(wide[tp, n], own_weight, preferred_element_type=f32)
        part = part + block(cp_ref, tp)[rows].astype(f32)
        for source in around:
            part = part + conv_in[source, rows].astype(f32)
        result.append(part)
    right_x, across_x, left_x = around

    def relay_final(n):
        return final_copy(left_x if n == 0 else right_x, n, relay_f.at[n], sides[n])

    def final_arrived(source, n):
        final_copy(source, n, relay_f.at[n], sides[n]).wait_recv()

    def take(source, n):
        result[n] = result[n] + jnp.dot(
            wide[source, n], weight_in[source], preferred_element_type=f32
        )

    final_arrived(left_x, 0)
    relay_final(0).start()
    final_arrived(right_x, 1)
    relay_final(1).start()
    take(left_x, 0)
    take(right_x, 1)
    final_arrived(left_x, 1)
    take(left_x, 1)
    final_arrived(right_x, 0)
    take(right_x, 0)
    for n in range(2):
        final_arrived(across_x, n)
        take(across_x, n)
        out_ref[n * half : (n + 1) * half, :] = result[n].astype(bf16)
    for copy in last:
        copy.wait_send()
    for n in range(2):
        relay_final(n).wait_send()


def attend(xp, qt, key_up, value_up, out_attend, glu, taps, bias, gain, out_conv, size):
    heads, width, own_q = qt.shape
    vdim = value_up.shape[1] // heads
    columns = out_attend.shape[1] // 4
    channels = glu.shape[1]
    vmem = pl.BlockSpec(memory_space=pltpu.VMEM)
    dma = pltpu.SemaphoreType.DMA
    scale = math.log2(math.e) * size ** (-0.5)
    return pl.pallas_call(
        functools.partial(attend_kernel, heads, scale),
        out_shape=jax.ShapeDtypeStruct((own_q, columns), bf16),
        in_specs=[vmem] * 10,
        out_specs=vmem,
        scratch_shapes=[
            pltpu.VMEM((8, *xp.shape), bf16),
            pltpu.VMEM((4, 2, heads, width, own_q), bf16),
            pltpu.VMEM((4, heads, 2 * own_q, width), bf16),
            pltpu.VMEM((4, heads, vdim + 16, 2 * own_q), bf16),
            pltpu.VMEM((4, heads, vdim + 16, 2 * own_q), f32),
            pltpu.VMEM((4, heads, 2 * own_q), f32),
            pltpu.VMEM((4, heads, vdim + 16, own_q), f32),
            pltpu.VMEM((4, heads, own_q), f32),
            pltpu.VMEM((3, heads, vdim, own_q), bf16),
            pltpu.VMEM((3, heads, 8, own_q), f32),
            pltpu.VMEM((3, heads, vdim, own_q), bf16),
            pltpu.VMEM((3, heads, 8, own_q), f32),
            pltpu.VMEM((4, 2, own_q // 2, heads * vdim), bf16),
            pltpu.VMEM((4, own_q, columns), bf16),
            pltpu.VMEM((4, heads * vdim, columns), bf16),
            pltpu.VMEM((2, 16, channels), bf16),
            pltpu.VMEM((own_q + 32, channels), f32),
            pltpu.VMEM((own_q + 8, 128), f32),
            pltpu.VMEM((own_q, channels), f32),
            pltpu.VMEM((4, 8, own_q), f32),
            pltpu.VMEM((own_q, channels), bf16),
            pltpu.VMEM((own_q, 4 * columns), bf16),
            pltpu.VMEM(value_up.shape[::-1], bf16),
            dma((8, 2)),
            dma((8, 2)),
            dma((4, 2)),
            dma((2, 2)),
            dma((2,)),
            dma((4, 2)),
            dma((4, 2)),
            dma((4, 4)),
            dma((3, 2, 2)),
            dma((2, 3)),
            dma((2, 4)),
            dma((2, 2)),
            dma((3,)),
            dma((4,)),
            dma((2, 2)),
            dma((4, 2)),
            dma((2,)),
        ],
        compiler_params=pltpu.CompilerParams(
            collective_id=0, has_side_effects=True, vmem_limit_bytes=40 * 2**20
        ),
        cost_estimate=pl.CostEstimate(
            flops=2 * 8192 * 2 * own_q * heads * 320,
            bytes_accessed=2 * 10**6,
            transcendentals=8192 * 2 * own_q * heads,
        ),
        name="attend",
    )(xp, qt, key_up, value_up, out_attend, glu, taps, bias[None], gain[None], out_conv)


def project_kernel(
    tok_ref, gain_ref, qg_ref, lg_ref, wq_ref, wl_ref, wr_ref, wv_ref, wg_ref,
    q_ref, kv_ref, rope_ref, glu_ref,
    blocks, wq, wl, wr, wv, wg, aq, al, ar, av, ag, squares,
    sent, got, sent_relay, local,
):
    sp, tp = lax.axis_index("sp"), lax.axis_index("tp")
    width = tok_ref.shape[2]
    half = tok_ref.shape[1]

    def turn(a):
        return lax.rem(a + 4, 4)

    sides = [(sp, turn(tp + 1)), (sp, turn(tp - 1))]
    barrier = pltpu.get_barrier_semaphore()
    for peer in sides:
        pl.semaphore_signal(barrier, inc=1, device_id=peer, device_id_type=pl.DeviceIdType.MESH)
    pl.semaphore_wait(barrier, 2)

    def remote(src, at, n, sem, target):
        return pltpu.make_async_remote_copy(
            src_ref=src, dst_ref=blocks.at[at, n], send_sem=sem, recv_sem=got.at[at, n],
            device_id=target, device_id_type=pl.DeviceIdType.MESH,
        )

    first = [
        remote(tok_ref.at[m], tp, m, sent.at[way, m], sides[way])
        for n in range(2)
        for way, m in ((0, n), (1, 1 - n))
    ]
    for copy in first:
        copy.start()
    loads = [
        pltpu.make_async_copy(a, b, local.at[i])
        for i, (a, b) in enumerate(
            ((wq_ref, wq), (wl_ref, wl), (wr_ref, wr), (wv_ref, wv), (wg_ref, wg))
        )
    ]
    for copy in loads:
        copy.start()

    def relay(n):
        source = turn(tp - 1 + 2 * n)
        return remote(blocks.at[source, n], source, n, sent_relay.at[n], sides[n])

    def arrived(offset, n):
        source = turn(tp + offset)
        remote(blocks.at[source, n], source, n, sent_relay.at[n], sides[n]).wait_recv()

    def add(source, piece, n, fresh):
        here = slice(n * half, (n + 1) * half)
        value = piece.astype(f32)
        scaled = (value * gain_ref[source]).astype(bf16)
        square = jnp.broadcast_to(jnp.sum(value * value, axis=1, keepdims=True), (half, 128))
        rows = pl.ds(pl.multiple_of(source * width, width), width)
        squares[here] = square if fresh else squares[here] + square
        for w, a in ((wq, aq), (wl, al), (wr, ar), (wv, av), (wg, ag)):
            if w is wr:
                part = lax.dot_general(
                    scaled, w[:, rows], (((1,), (1,)), ((), ())), preferred_element_type=f32
                )
            else:
                part = jnp.dot(scaled, w[rows, :], preferred_element_type=f32)
            a[here] = part if fresh else a[here] + part

    for copy in loads:
        copy.wait()
    for n in range(2):
        add(tp, tok_ref[n], n, True)
    arrived(-1, 0)
    relay(0).start()
    arrived(1, 1)
    relay(1).start()
    left, right, across = turn(tp - 1), turn(tp + 1), turn(tp + 2)
    add(left, blocks[left, 0], 0, False)
    add(right, blocks[right, 1], 1, False)
    arrived(-1, 1)
    add(left, blocks[left, 1], 1, False)
    arrived(1, 0)
    add(right, blocks[right, 0], 0, False)
    for n in range(2):
        arrived(2, n)
        add(across, blocks[across, n], n, False)
    row_scale = lax.rsqrt(squares[:, :1] / (4 * width) + eps_norm)
    q_ref[...] = rms_scale(row_scale * aq[...], qg_ref[...]).astype(bf16)
    kv_ref[...] = rms_scale(row_scale * al[...], lg_ref[...]).astype(bf16)
    rope_ref[...] = row_scale * ar[...]
    glu_ref[...] = (row_scale * av[...] * jax.nn.sigmoid(row_scale * ag[...])).astype(bf16)
    for copy in first:
        copy.wait_send()
    for n in range(2):
        relay(n).wait_send()


def project(tokens, in_gain, query_gain, latent_gain, weights):
    rows, width = tokens.shape
    vmem = pl.BlockSpec(memory_space=pltpu.VMEM)
    dma = pltpu.SemaphoreType.DMA
    wide = [min(w.shape) for w in weights]
    return pl.pallas_call(
        project_kernel,
        out_shape=(
            jax.ShapeDtypeStruct((rows, wide[0]), bf16),
            jax.ShapeDtypeStruct((rows, wide[1]), bf16),
            jax.ShapeDtypeStruct((rows, wide[2]), f32),
            jax.ShapeDtypeStruct((rows, wide[3]), bf16),
        ),
        in_specs=[vmem] * 4 + [pl.BlockSpec(memory_space=pl.ANY)] * 5,
        out_specs=(vmem,) * 4,
        scratch_shapes=[pltpu.VMEM((4, 2, rows // 2, width), bf16)]
        + [pltpu.VMEM(w.shape, bf16) for w in weights]
        + [pltpu.VMEM((rows, n), f32) for n in wide]
        + [pltpu.VMEM((rows, 128), f32), dma((2, 2)), dma((4, 2)), dma((2,)), dma((5,))],
        compiler_params=pltpu.CompilerParams(
            collective_id=1, has_side_effects=True, vmem_limit_bytes=60 * 2**20
        ),
        cost_estimate=pl.CostEstimate(
            flops=2 * rows * 4 * width * sum(wide), bytes_accessed=10**7, transcendentals=10**5
        ),
        name="project",
    )(
        tokens.reshape(2, rows // 2, width),
        in_gain.reshape(4, 1, width),
        query_gain[None],
        latent_gain[None],
        *weights,
    )


def per_device(
    tokens,
    in_gain,
    query_down,
    latent_down,
    rope_down,
    query_gain,
    latent_gain,
    query_nope,
    query_rope,
    key_up,
    value_up,
    conv_value,
    conv_gate,
    conv_taps,
    conv_bias,
    channel_gain,
    out_attend,
    out_conv,
):
    row_count = tokens.shape[0]
    positions = (lax.axis_index("sp") * row_count + jnp.arange(row_count)).astype(f32)
    q_latent, kv_latent, rope_pre, glu = project(
        tokens,
        in_gain,
        query_gain,
        latent_gain,
        (query_down, latent_down, jnp.transpose(rope_down), conv_value, conv_gate),
    )
    rope_key = rotate(rope_pre, positions).astype(bf16)
    rope_size = rope_down.shape[1]
    heads = query_rope.shape[1] // rope_size
    nope = query_nope.shape[1] // heads

    packed = jnp.transpose(rope_key.reshape(2, 8, 16, rope_size), (0, 2, 1, 3)).reshape(2, 16, 8 * rope_size)
    xp = jnp.concatenate([kv_latent.reshape(2, row_count // 2, -1), packed], axis=1)

    q_heads = (
        jnp.dot(q_latent, query_nope, preferred_element_type=f32)
        .astype(bf16)
        .reshape(row_count, heads, nope)
    )
    q_turn = jnp.dot(q_latent, query_rope, preferred_element_type=f32).reshape(
        row_count, heads, rope_size
    )
    r_heads = rotate(q_turn, positions[:, None]).astype(bf16)
    empty = jnp.zeros((row_count, 64 - rope_size), bf16)
    cols = []
    for h in range(heads):
        if h % 2 == 0:
            cols += [q_heads[:, h], r_heads[:, h], empty]
        else:
            cols += [r_heads[:, h], empty, q_heads[:, h]]
    q_own = jnp.transpose(jnp.concatenate(cols, axis=1))
    return attend(
        xp,
        q_own.reshape(heads, 128, row_count),
        key_up,
        value_up,
        out_attend,
        glu,
        conv_taps,
        conv_bias,
        channel_gain,
        out_conv,
        nope + rope_size,
    )


def solution(mesh):
    in_specs = (
        P("sp", "tp"),
        P(),
        P(),
        P(),
        P(),
        P(),
        P(),
        P(None, "tp"),
        P(None, "tp"),
        P(None, "tp"),
        P(None, "tp"),
        P(None, "tp"),
        P(None, "tp"),
        P(None, "tp"),
        P("tp"),
        P("tp"),
        P("tp", None),
        P("tp", None),
    )
    return jax.shard_map(
        per_device, mesh=mesh, in_specs=in_specs, out_specs=P("sp", "tp"), check_vma=False
    )
```

```python
import functools
import math

import jax
import jax.numpy as jnp
from jax import lax
from jax.experimental import pallas as pl
from jax.experimental.pallas import tpu as pltpu
from jax.sharding import PartitionSpec as P

eps_norm = 1e-06
eps_layer = 1e-05
theta = 10000.0
bf16 = jnp.bfloat16
f32 = jnp.float32

def rms_scale(values, gain):
    return values * lax.rsqrt(jnp.mean(values * values, axis=-1, keepdims=True) + eps_norm) * gain


def rotate(values, cosine, sine):
    half = values.shape[-1] // 2
    first = values[..., :half]
    second = values[..., half:]
    return jnp.concatenate(
        [first * cosine - second * sine, second * cosine + first * sine], axis=-1
    )


def attend_kernel(
    heads, scale, xp_ref, qt_ref, ku_ref, vu_ref, wa_ref, glu_ref,
    taps_ref, bias_ref, gain_ref, oc_ref, out_ref,
    x, q, keys, vals, acc, high, acc_in, high_in, part_out, stat_out, part_in, stat_in, wide, conv_in, weight_in,
    halo, padded, shifted, conv, moments, active, cp_ref, vut_ref,
    got_x, sent_x, got_q, sent_q, sent_relay, sent_pair_q, got_pair_q, pair_sem, part_sem,
    sent_t, got_t, halo_sem, sent_m, got_m, sent_f, got_f, relay_f,
):
    sp, tp = lax.axis_index("sp"), lax.axis_index("tp")
    core = lax.rem(sp, 2)
    y = lax.rem(sp // 2, 4)
    z = sp // 8
    own_q = qt_ref.shape[2]
    depth = xp_ref.shape[1] - 16
    vrows = vu_ref.shape[1] // heads
    half_heads = heads // 2

    def device(pz, py):
        return (((pz * 4 + py) * 2 + core), tp)

    def turn(a, n):
        return lax.rem(a + 2 * n, n)

    up, down = device(turn(z + 1, 8), y), device(turn(z - 1, 8), y)
    right, left = device(z, turn(y + 1, 4)), device(z, turn(y - 1, 4))
    across = device(z, turn(y + 2, 4))
    sibling = (sp + 1 - 2 * core, tp)

    def remote(src, dst, sent, got, target):
        return pltpu.make_async_remote_copy(
            src_ref=src, dst_ref=dst, send_sem=sent, recv_sem=got,
            device_id=target, device_id_type=pl.DeviceIdType.MESH,
        )

    barrier = pltpu.get_barrier_semaphore()
    others = [(sp, lax.rem(tp + i, 4)) for i in (1, 3, 2)]
    count = 64
    beside = [(lax.rem(sp + 1, count), tp), (lax.rem(sp + count - 1, count), tp)]
    peers = (up, down, right, left, across, sibling, *others, *beside)
    for peer in peers:
        pl.semaphore_signal(barrier, inc=1, device_id=peer, device_id_type=pl.DeviceIdType.MESH)
    pl.semaphore_wait(barrier, len(peers))

    def plane(k):
        return turn(z + (1 - 2 * lax.rem(k, 2)) * ((k + 1) // 2), 8)

    def x_copy(k, n, target):
        at = x.at[plane(k), n]
        return remote(at, at, sent_x.at[k, n], got_x.at[plane(k), n], target)

    def part_of(ref, n):
        return ref.at[n * half_heads : (n + 1) * half_heads]

    def q_slot(py, who, n):
        return q.at[py, who, n * half_heads : (n + 1) * half_heads]

    first = []
    for n in range(2):
        for way, target in enumerate((up, down)):
            first.append(
                remote(xp_ref.at[n], x.at[z, n], sent_x.at[7 * way, n], got_x.at[z, n], target)
            )
    for n in range(2):
        for way, target in enumerate((right, left)):
            m = n if way == 0 else 1 - n
            first.append(
                remote(part_of(qt_ref, m), q_slot(y, core, m), sent_q.at[way, m], got_q.at[y, m], target)
            )
    for n in range(2):
        first.append(
            remote(
                part_of(qt_ref, n), q_slot(y, core, n), sent_pair_q.at[0, n],
                got_pair_q.at[y, n], sibling,
            )
        )
    columns = out_ref.shape[1]

    def block(ref, n):
        return ref.at[:, pl.ds(pl.multiple_of(n * columns, columns), columns)]

    def block_copy(kind, i, src, dst):
        peer = others[i]
        return remote(block(src, peer[1]), dst.at[tp], sent_t.at[kind, i], got_t.at[kind, tp], peer)

    halos = [
        remote(
            glu_ref.at[own_q - 16 :] if n == 0 else glu_ref.at[:16],
            halo.at[n], halo_sem.at[n, 0], halo_sem.at[n, 1], beside[n],
        )
        for n in range(2)
    ]
    first = halos + first + [block_copy(0, i, wa_ref, weight_in) for i in range(3)]
    for copy in first:
        copy.start()
    x[z] = xp_ref[...]
    q[y, core] = qt_ref[...]
    vut_ref[...] = jnp.transpose(vu_ref[...].astype(f32)).astype(bf16)
    acc[...] = jnp.zeros_like(acc)
    high[...] = jnp.full_like(high, -jnp.inf)

    def goes(k, n):
        return k < 5 or (k == 5 and n == 0) or (k == 6 and n == 1)

    def x_first(k):
        for n in range(2):
            copy = x_copy(k, n, up if k % 2 else down)
            copy.wait_recv()
            if goes(k, n):
                copy.start()

    def pair_q(r, n):
        py = turn(y + r, 4)
        at = q_slot(py, core, n)
        return remote(at, at, sent_pair_q.at[r, n], got_pair_q.at[py, n], sibling)

    def arrived_q(r, n):
        py = turn(y + r, 4)
        at = q_slot(py, core, n)
        remote(at, at, sent_relay.at[n], got_q.at[py, n], sibling).wait_recv()

    def relay_q(n):
        py = turn(y - 1 + 2 * n, 4)
        at = q_slot(py, core, n)
        return remote(at, at, sent_relay.at[n], got_q.at[py, n], right if n == 0 else left)

    def pair_arrived(r):
        py = turn(y + r, 4)
        for n in range(2):
            at = q_slot(py, 1 - core, n)
            remote(at, at, sent_relay.at[n], got_pair_q.at[py, n], sibling).wait_recv()

    def q_from(r, order):
        for n in order:
            arrived_q(r, n)
            if (r, n) in ((3, 0), (1, 1)):
                relay_q(n).start()
            pair_q(r, n).start()

    def swap(r):
        return [
            remote(
                acc.at[r, :, :, own_q:], acc_in.at[r], pair_sem.at[r, 0], pair_sem.at[r, 1], sibling
            ),
            remote(high.at[r, :, own_q:], high_in.at[r], pair_sem.at[r, 2], pair_sem.at[r, 3], sibling),
        ]

    def swap_start(r):
        for copy in swap(r):
            copy.start()

    def part_copy(r):
        return [
            remote(
                out.at[r - 1], into.at[r - 1], part_sem.at[r - 1, n, 0], part_sem.at[r - 1, n, 1],
                {1: right, 2: across, 3: left}[r],
            )
            for n, (out, into) in enumerate(((stat_out, stat_in), (part_out, part_in)))
        ]

    def merge(r):
        for copy in swap(r):
            copy.wait()
        for h in range(heads):
            m0, m1 = high[r, h : h + 1, :own_q], high_in[r, h : h + 1, :]
            top = jnp.maximum(m0, m1)
            a0, a1 = jnp.exp2((m0 - top) * scale), jnp.exp2((m1 - top) * scale)
            total = acc[r, h, vrows : vrows + 1, :own_q] * a0 + acc_in[r, h, vrows : vrows + 1, :] * a1
            whole = acc[r, h, :vrows, :own_q] * a0 + acc_in[r, h, :vrows, :] * a1
            part_out[r - 1, h] = (whole / total).astype(bf16)
            stat_out[r - 1, h] = jnp.concatenate([total] * 4 + [top] * 4, axis=0)
        for copy in part_copy(r):
            copy.start()

    def expand(c):
        at = [plane(2 * c), plane(2 * c + 1)]
        latent = jnp.concatenate([x[s, n, :depth, :] for s in at for n in range(2)], axis=0)
        k = jnp.dot(latent, ku_ref[...], preferred_element_type=f32).astype(bf16)
        vt = lax.dot_general(
            vut_ref[...], latent, (((1,), (1,)), ((), ())), preferred_element_type=f32
        ).astype(bf16)
        even, odd = [], []
        for s in at:
            for n in range(2):
                for half in range(2):
                    part = x[s, n, depth:, 128 * half : 128 * half + 128].astype(f32)
                    r1, r2, r3 = (pltpu.roll(part, 32 * m, 1) for m in (1, 2, 3))
                    even += [r2, r1, part, r3]
                    odd += [part, r3, r2, r1]
        even = jnp.concatenate(even, axis=0).astype(bf16)
        odd = jnp.concatenate(odd, axis=0).astype(bf16)
        lane = lax.broadcasted_iota(jnp.int32, even.shape, 1)
        for h in range(heads):
            pair = k[:, 128 * (h // 2) : 128 * (h // 2) + 128]
            keys[c, h] = (
                jnp.where(lane < 64, pair, even) if h % 2 == 0 else jnp.where(lane >= 64, pair, odd)
            )
            vals[c, h, :vrows, :] = vt[h * vrows : (h + 1) * vrows]
            vals[c, h, vrows:, :] = jnp.ones((16, vt.shape[1]), bf16)

    def compute(r, c):
        py = turn(y + r, 4)

        def score(h):
            both = jnp.concatenate([q[py, core, h], q[py, 1 - core, h]], axis=1)
            return jnp.dot(keys[c, h], both, preferred_element_type=f32)

        following = score(0)
        for h in range(heads):
            s = following
            if h + 1 < heads:
                following = score(h + 1)
            old = high[r, h : h + 1, :]
            new = jnp.maximum(old, jnp.max(s, axis=0, keepdims=True))
            alpha = jnp.exp2((old - new) * scale)
            p = jnp.exp2((s - new) * scale).astype(bf16)
            high[r, h : h + 1, :] = new
            acc[r, h] = acc[r, h] * alpha + jnp.dot(vals[c, h], p, preferred_element_type=f32)

    channels = glu_ref.shape[1]

    def convolve():
        for copy in halos:
            copy.wait_recv()
        padded[16 : 16 + own_q, :] = glu_ref[...].astype(f32)
        padded[:16, :] = jnp.where(sp > 0, halo[0].astype(f32), 0.0)
        padded[16 + own_q :, :] = jnp.where(sp < count - 1, halo[1].astype(f32), 0.0)
        taps = taps_ref.shape[0]
        for at in range(0, channels, 128):
            lanes = slice(at, at + 128)
            total = jnp.broadcast_to(bias_ref[:, lanes], (own_q, 128))
            for r in range(8):
                part = None
                for j in range(4):
                    k = 8 * j + r - 1
                    if 0 <= k < taps:
                        term = taps_ref[k : k + 1, lanes] * padded[8 * j : 8 * j + own_q + 8, lanes]
                        part = term if part is None else part + term
                shifted[...] = part
                total = total + shifted[r : r + own_q, :]
            conv[:, lanes] = total
        whole = conv[...]
        mean = jnp.sum(whole, axis=1, keepdims=True) / channels
        off = whole - mean
        spread = jnp.sum(off * off, axis=1, keepdims=True)
        lane = lax.broadcasted_iota(jnp.int32, (own_q, 128), 1)
        moments[tp] = jnp.transpose(jnp.where(lane == 0, mean, spread))[:8]

    def moment_copy(i):
        at = moments.at[tp]
        return remote(at, at, sent_m.at[i], got_m.at[tp], others[i])

    def activate():
        for i in range(1, 4):
            source = lax.rem(tp + i, 4)
            at = moments.at[source]
            remote(at, at, sent_m.at[0], got_m.at[source], others[0]).wait_recv()
        means = [moments[n, 0:1, :] for n in range(4)]
        mean = sum(means) / 4
        apart = sum((m - mean) * (m - mean) for m in means)
        spread = (sum(moments[n, 1:2, :] for n in range(4)) + channels * apart) / (4 * channels)
        tall = lambda row: jnp.transpose(jnp.broadcast_to(row, (128, own_q)))
        mean, scaling = tall(mean), tall(lax.rsqrt(spread + eps_layer))
        for at in range(0, channels, 128):
            lanes = slice(at, at + 128)
            value = (conv[:, lanes] - mean) * scaling * gain_ref[:, lanes]
            active[:, lanes] = jax.nn.silu(value).astype(bf16)
        for n in range(4):
            cols = slice(n * columns, (n + 1) * columns)
            cp_ref[:, cols] = jnp.dot(
                active[...], oc_ref[:, cols], preferred_element_type=f32
            ).astype(bf16)

    convolve()
    x_first(1)
    x_first(2)
    for i in range(3):
        moment_copy(i).start()
    expand(0)
    q_from(1, (1, 0))
    q_from(3, (0, 1))
    activate()
    x_first(3)
    x_first(4)
    for i in range(3):
        block_copy(1, i, cp_ref, conv_in).start()
    pair_arrived(0)

    blocks = (0, 1, 3, 1, 3, 1, 1, 2, 2, 2, 2, 3, 3, 0, 0, 0)
    chunks = (0, 0, 0, 1, 1, 2, 3, 0, 1, 2, 3, 2, 3, 1, 2, 3)

    def looked_up(step, values):
        found = values[0]
        for n in range(1, 16):
            if values[n] != values[n - 1]:
                found = found + (values[n] - values[n - 1]) * ((step + 16 - n) // 16)
        return found

    hooks = {
        1: lambda: pair_arrived(1),
        2: lambda: pair_arrived(3),
        3: lambda: (x_first(5), x_first(6), q_from(2, (0, 1)), expand(1)),
        5: lambda: (x_first(7), expand(2)),
        6: lambda: expand(3),
        7: lambda: (pair_arrived(2), swap_start(1)),
        8: lambda: merge(1),
        11: lambda: swap_start(2),
        12: lambda: merge(2),
        13: lambda: swap_start(3),
        14: lambda: merge(3),
    }

    @pl.loop(0, 16)
    def _(step):
        for n, hook in hooks.items():
            def run(hook=hook):
                hook()
            pl.when(step == n)(run)
        compute(looked_up(step, blocks), looked_up(step, chunks))

    swap_start(0)
    for copy in first:
        copy.wait_send()
    for i in range(3):
        moment_copy(i).wait_send()
        block_copy(1, i, cp_ref, conv_in).wait_send()
    for k in range(1, 8):
        for n in range(2):
            if goes(k, n):
                x_copy(k, n, up if k % 2 else down).wait_send()
    for n in range(2):
        relay_q(n).wait_send()
        for r in range(1, 4):
            pair_q(r, n).wait_send()
    for r in range(1, 4):
        for copy in part_copy(r):
            copy.wait()
    for copy in swap(0):
        copy.wait()
    half = own_q // 2
    for h in range(heads):
        tops = [high[0, h : h + 1, :own_q], high_in[0, h : h + 1, :]]
        totals = [acc[0, h, vrows : vrows + 1, :own_q], acc_in[0, h, vrows : vrows + 1, :]]
        for r in range(3):
            tops.append(stat_in[r, h, 4:5, :])
            totals.append(stat_in[r, h, 0:1, :])
        top = functools.reduce(jnp.maximum, tops)
        shares = [jnp.exp2((m - top) * scale) for m in tops]
        total = sum(t * a for t, a in zip(totals, shares))
        whole = acc[0, h, :vrows, :own_q] * shares[0] + acc_in[0, h, :vrows, :] * shares[1]
        for r in range(3):
            whole = whole + part_in[r, h].astype(f32) * (shares[2 + r] * totals[2 + r])
        done = jnp.transpose(whole / total).astype(bf16)
        for n in range(2):
            wide[tp, n, :, h * vrows : (h + 1) * vrows] = done[n * half : (n + 1) * half]
    def final_copy(source, n, sem, target):
        at = wide.at[source, n]
        return remote(at, at, sem, got_f.at[source, n], target)

    sides = others[:2]
    last = [
        final_copy(tp, m, sent_f.at[way, m], sides[way])
        for n in range(2)
        for way, m in ((0, n), (1, 1 - n))
    ]
    for copy in last:
        copy.start()
    own_weight = block(wa_ref, tp)[...]
    around = [lax.rem(tp + i, 4) for i in (1, 2, 3)]
    for source in around:
        for kind, dst in enumerate((weight_in, conv_in)):
            at = dst.at[source]
            remote(at, at, sent_t.at[kind, 0], got_t.at[kind, source], others[0]).wait_recv()
    result = []
    for n in range(2):
        rows = slice(n * half, (n + 1) * half)
        part = jnp.dot(wide[tp, n], own_weight, preferred_element_type=f32)
        part = part + block(cp_ref, tp)[rows].astype(f32)
        for source in around:
            part = part + conv_in[source, rows].astype(f32)
        result.append(part)
    right_x, across_x, left_x = around

    def relay_final(n):
        return final_copy(left_x if n == 0 else right_x, n, relay_f.at[n], sides[n])

    def final_arrived(source, n):
        final_copy(source, n, relay_f.at[n], sides[n]).wait_recv()

    def take(source, n):
        result[n] = result[n] + jnp.dot(
            wide[source, n], weight_in[source], preferred_element_type=f32
        )

    final_arrived(left_x, 0)
    relay_final(0).start()
    final_arrived(right_x, 1)
    relay_final(1).start()
    take(left_x, 0)
    take(right_x, 1)
    final_arrived(left_x, 1)
    take(left_x, 1)
    final_arrived(right_x, 0)
    take(right_x, 0)
    for n in range(2):
        final_arrived(across_x, n)
        take(across_x, n)
        out_ref[n * half : (n + 1) * half, :] = result[n].astype(bf16)
    for copy in last:
        copy.wait_send()
    for n in range(2):
        relay_final(n).wait_send()


def attend(xp, qt, key_up, value_up, out_attend, glu, taps, bias, gain, out_conv, size):
    heads, width, own_q = qt.shape
    vdim = value_up.shape[1] // heads
    columns = out_attend.shape[1] // 4
    channels = glu.shape[1]
    vmem = pl.BlockSpec(memory_space=pltpu.VMEM)
    dma = pltpu.SemaphoreType.DMA
    scale = math.log2(math.e) * size ** (-0.5)
    return pl.pallas_call(
        functools.partial(attend_kernel, heads, scale),
        out_shape=jax.ShapeDtypeStruct((own_q, columns), bf16),
        in_specs=[vmem] * 10,
        out_specs=vmem,
        scratch_shapes=[
            pltpu.VMEM((8, *xp.shape), bf16),
            pltpu.VMEM((4, 2, heads, width, own_q), bf16),
            pltpu.VMEM((4, heads, 2 * own_q, width), bf16),
            pltpu.VMEM((4, heads, vdim + 16, 2 * own_q), bf16),
            pltpu.VMEM((4, heads, vdim + 16, 2 * own_q), f32),
            pltpu.VMEM((4, heads, 2 * own_q), f32),
            pltpu.VMEM((4, heads, vdim + 16, own_q), f32),
            pltpu.VMEM((4, heads, own_q), f32),
            pltpu.VMEM((3, heads, vdim, own_q), bf16),
            pltpu.VMEM((3, heads, 8, own_q), f32),
            pltpu.VMEM((3, heads, vdim, own_q), bf16),
            pltpu.VMEM((3, heads, 8, own_q), f32),
            pltpu.VMEM((4, 2, own_q // 2, heads * vdim), bf16),
            pltpu.VMEM((4, own_q, columns), bf16),
            pltpu.VMEM((4, heads * vdim, columns), bf16),
            pltpu.VMEM((2, 16, channels), bf16),
            pltpu.VMEM((own_q + 32, channels), f32),
            pltpu.VMEM((own_q + 8, 128), f32),
            pltpu.VMEM((own_q, channels), f32),
            pltpu.VMEM((4, 8, own_q), f32),
            pltpu.VMEM((own_q, channels), bf16),
            pltpu.VMEM((own_q, 4 * columns), bf16),
            pltpu.VMEM(value_up.shape[::-1], bf16),
            dma((8, 2)),
            dma((8, 2)),
            dma((4, 2)),
            dma((2, 2)),
            dma((2,)),
            dma((4, 2)),
            dma((4, 2)),
            dma((4, 4)),
            dma((3, 2, 2)),
            dma((2, 3)),
            dma((2, 4)),
            dma((2, 2)),
            dma((3,)),
            dma((4,)),
            dma((2, 2)),
            dma((4, 2)),
            dma((2,)),
        ],
        compiler_params=pltpu.CompilerParams(
            collective_id=0, has_side_effects=True, vmem_limit_bytes=40 * 2**20
        ),
        cost_estimate=pl.CostEstimate(
            flops=2 * 8192 * 2 * own_q * heads * 320,
            bytes_accessed=2 * 10**6,
            transcendentals=8192 * 2 * own_q * heads,
        ),
        name="attend",
    )(xp, qt, key_up, value_up, out_attend, glu, taps, bias[None], gain[None], out_conv)


def project_kernel(
    tok_ref, gain_ref, qg_ref, lg_ref, freq_ref,
    wq_ref, wl_ref, wr_ref, wv_ref, wg_ref, wn_ref, wt_ref,
    qt_ref, kv_ref, rope_ref, glu_ref, cos_ref, sin_ref,
    blocks, wq, wl, wr, wv, wg, wn, wt, aq, al, ar, av, ag, squares,
    sent, got, sent_relay, local,
):
    sp, tp = lax.axis_index("sp"), lax.axis_index("tp")
    width = tok_ref.shape[2]
    half = tok_ref.shape[1]

    def turn(a):
        return lax.rem(a + 4, 4)

    sides = [(sp, turn(tp + 1)), (sp, turn(tp - 1))]
    barrier = pltpu.get_barrier_semaphore()
    for peer in sides:
        pl.semaphore_signal(barrier, inc=1, device_id=peer, device_id_type=pl.DeviceIdType.MESH)
    pl.semaphore_wait(barrier, 2)

    def remote(src, at, n, sem, target):
        return pltpu.make_async_remote_copy(
            src_ref=src, dst_ref=blocks.at[at, n], send_sem=sem, recv_sem=got.at[at, n],
            device_id=target, device_id_type=pl.DeviceIdType.MESH,
        )

    first = [
        remote(tok_ref.at[m], tp, m, sent.at[way, m], sides[way])
        for n in range(2)
        for way, m in ((0, n), (1, 1 - n))
    ]
    for copy in first:
        copy.start()
    loads = [
        pltpu.make_async_copy(a, b, local.at[i])
        for i, (a, b) in enumerate(
            (
                (wq_ref, wq), (wl_ref, wl), (wr_ref, wr), (wv_ref, wv), (wg_ref, wg),
                (wn_ref, wn), (wt_ref, wt),
            )
        )
    ]
    for copy in loads:
        copy.start()

    def relay(n):
        source = turn(tp - 1 + 2 * n)
        return remote(blocks.at[source, n], source, n, sent_relay.at[n], sides[n])

    def arrived(offset, n):
        source = turn(tp + offset)
        remote(blocks.at[source, n], source, n, sent_relay.at[n], sides[n]).wait_recv()

    def add(source, piece, n, fresh):
        here = slice(n * half, (n + 1) * half)
        value = piece.astype(f32)
        scaled = (value * gain_ref[source]).astype(bf16)
        square = jnp.broadcast_to(jnp.sum(value * value, axis=1, keepdims=True), (half, 128))
        rows = pl.ds(pl.multiple_of(source * width, width), width)
        squares[here] = square if fresh else squares[here] + square
        for w, a in ((wq, aq), (wl, al), (wr, ar), (wv, av), (wg, ag)):
            if w is wr:
                part = lax.dot_general(
                    scaled, w[:, rows], (((1,), (1,)), ((), ())), preferred_element_type=f32
                )
            else:
                part = jnp.dot(scaled, w[rows, :], preferred_element_type=f32)
            a[here] = part if fresh else a[here] + part

    place = sp * cos_ref.shape[1] + lax.broadcasted_iota(jnp.int32, cos_ref.shape, 1)
    angles = freq_ref[...] * place.astype(f32)
    cos_ref[...] = jnp.cos(angles)
    sin_ref[...] = jnp.sin(angles)
    for copy in loads:
        copy.wait()
    for n in range(2):
        add(tp, tok_ref[n], n, True)
    arrived(-1, 0)
    relay(0).start()
    arrived(1, 1)
    relay(1).start()
    left, right, across = turn(tp - 1), turn(tp + 1), turn(tp + 2)
    add(left, blocks[left, 0], 0, False)
    add(right, blocks[right, 1], 1, False)
    arrived(-1, 1)
    add(left, blocks[left, 1], 1, False)
    arrived(1, 0)
    add(right, blocks[right, 0], 0, False)
    for n in range(2):
        arrived(2, n)
        add(across, blocks[across, n], n, False)
    row_scale = lax.rsqrt(squares[:, :1] / (4 * width) + eps_norm)
    latent = rms_scale(row_scale * aq[...], qg_ref[...]).astype(bf16)
    plain = jnp.transpose(jnp.dot(latent, wn[...], preferred_element_type=f32)).astype(bf16)
    turned = jnp.transpose(jnp.dot(latent, wt[...], preferred_element_type=f32))
    heads = qt_ref.shape[0]
    nope, both = plain.shape[0] // heads, turned.shape[0] // heads
    cosine, sine = cos_ref[...], sin_ref[...]
    for h in range(heads):
        one = turned[h * both : h * both + both // 2]
        two = turned[h * both + both // 2 : (h + 1) * both]
        parts = [
            plain[h * nope : (h + 1) * nope],
            (one * cosine - two * sine).astype(bf16),
            (two * cosine + one * sine).astype(bf16),
            jnp.zeros((nope - both, plain.shape[1]), bf16),
        ]
        at = 0
        for part in parts if h % 2 == 0 else parts[1:] + parts[:1]:
            qt_ref[h, at : at + part.shape[0], :] = part
            at += part.shape[0]
    kv_ref[...] = rms_scale(row_scale * al[...], lg_ref[...]).astype(bf16)
    rope_ref[...] = row_scale * ar[...]
    glu_ref[...] = (row_scale * av[...] * jax.nn.sigmoid(row_scale * ag[...])).astype(bf16)
    for copy in first:
        copy.wait_send()
    for n in range(2):
        relay(n).wait_send()


def project(tokens, in_gain, query_gain, latent_gain, freqs, weights):
    rows, width = tokens.shape
    vmem = pl.BlockSpec(memory_space=pltpu.VMEM)
    dma = pltpu.SemaphoreType.DMA
    wide = [min(w.shape) for w in weights[:5]]
    half = freqs.shape[0]
    return pl.pallas_call(
        project_kernel,
        out_shape=(
            jax.ShapeDtypeStruct((weights[6].shape[1] // (2 * half), 128, rows), bf16),
            jax.ShapeDtypeStruct((rows, wide[1]), bf16),
            jax.ShapeDtypeStruct((rows, wide[2]), f32),
            jax.ShapeDtypeStruct((rows, wide[3]), bf16),
            jax.ShapeDtypeStruct((half, rows), f32),
            jax.ShapeDtypeStruct((half, rows), f32),
        ),
        in_specs=[vmem] * 5 + [pl.BlockSpec(memory_space=pl.ANY)] * 7,
        out_specs=(vmem,) * 6,
        scratch_shapes=[pltpu.VMEM((4, 2, rows // 2, width), bf16)]
        + [pltpu.VMEM(w.shape, bf16) for w in weights]
        + [pltpu.VMEM((rows, n), f32) for n in wide]
        + [pltpu.VMEM((rows, 128), f32), dma((2, 2)), dma((4, 2)), dma((2,)), dma((7,))],
        compiler_params=pltpu.CompilerParams(
            collective_id=1, has_side_effects=True, vmem_limit_bytes=60 * 2**20
        ),
        cost_estimate=pl.CostEstimate(
            flops=2 * rows * 4 * width * sum(wide), bytes_accessed=10**7, transcendentals=10**5
        ),
        name="project",
    )(
        tokens.reshape(2, rows // 2, width),
        in_gain.reshape(4, 1, width),
        query_gain[None],
        latent_gain[None],
        freqs[:, None],
        *weights,
    )


def per_device(
    tokens,
    in_gain,
    query_down,
    latent_down,
    rope_down,
    query_gain,
    latent_gain,
    query_nope,
    query_rope,
    key_up,
    value_up,
    conv_value,
    conv_gate,
    conv_taps,
    conv_bias,
    channel_gain,
    out_attend,
    out_conv,
):
    row_count = tokens.shape[0]
    half = rope_down.shape[1] // 2
    freqs = theta ** (-jnp.arange(half).astype(f32) / half)
    qt, kv_latent, rope_pre, glu, cosine, sine = project(
        tokens,
        in_gain,
        query_gain,
        latent_gain,
        freqs,
        (
            query_down,
            latent_down,
            jnp.transpose(rope_down),
            conv_value,
            conv_gate,
            query_nope,
            query_rope,
        ),
    )
    cosine, sine = jnp.transpose(cosine), jnp.transpose(sine)
    rope_key = rotate(rope_pre, cosine, sine).astype(bf16)
    rope_size = rope_down.shape[1]
    heads = query_rope.shape[1] // rope_size
    nope = query_nope.shape[1] // heads

    packed = jnp.transpose(rope_key.reshape(2, 8, 16, rope_size), (0, 2, 1, 3)).reshape(2, 16, 8 * rope_size)
    xp = jnp.concatenate([kv_latent.reshape(2, row_count // 2, -1), packed], axis=1)

    return attend(
        xp,
        qt,
        key_up,
        value_up,
        out_attend,
        glu,
        conv_taps,
        conv_bias,
        channel_gain,
        out_conv,
        nope + rope_size,
    )


def solution(mesh):
    in_specs = (
        P("sp", "tp"),
        P(),
        P(),
        P(),
        P(),
        P(),
        P(),
        P(None, "tp"),
        P(None, "tp"),
        P(None, "tp"),
        P(None, "tp"),
        P(None, "tp"),
        P(None, "tp"),
        P(None, "tp"),
        P("tp"),
        P("tp"),
        P("tp", None),
        P("tp", None),
    )
    return jax.shard_map(
        per_device, mesh=mesh, in_specs=in_specs, out_specs=P("sp", "tp"), check_vma=False
    )
```
